32 devices in a mesh: sp: 8 (over z, x), tp: 4 (over y, core).
Axes of the slice: x: 2, y: 2, z: 4, core: 2. Of those that a mesh axis runs over, the one named last changes fastest.
Arguments:
- queries: bfloat16 [2560, 1024], P('sp', 'tp'), may hold values from -6.6 to 6.6
- key_matrix: bfloat16 [2560, 256], P('sp', 'tp'), may hold values from -6.6 to 6.6
- values: bfloat16 [2560, 256], P('sp', 'tp'), may hold values from -6 to 6
- query_gain: float32 [64], replicated, may hold values from 0.19 to 8
- key_norm_gain: float32 [64], replicated, may hold values from 0.19 to 8
- head_gain: float32 [1024], P('tp'), may hold values from 0.1 to 1.9
- out_proj: bfloat16 [1024, 2048], replicated, may hold values from -0.1875 to 0.1875
- residual: bfloat16 [2560, 2048], P('sp'), may hold values from -6 to 6
- ffn_gain: float32 [2048], replicated, may hold values from 0.1 to 1.9
- routes: int32 [2560, 4], P('sp'), may hold values from 0 to 31, all different within a row; in each aligned block of 320 rows (0 to 319, 320 to 639, ...) at most 80 rows name the same one
- route_weights: float32 [2560, 4], P('sp'), may hold values from 0.2 to 1
- expert_gate: bfloat16 [32, 2048, 512], P(('sp', 'tp')), may hold values from -0.125 to 0.125
- expert_up: bfloat16 [32, 2048, 512], P(('sp', 'tp')), may hold values from -0.125 to 0.125
- expert_down: bfloat16 [32, 512, 2048], P(('sp', 'tp')), may hold values from -0.25 to 0.25
- shared_gate: bfloat16 [2048, 512], P(None, 'tp'), may hold values from -0.125 to 0.125
- shared_up: bfloat16 [2048, 512], P(None, 'tp'), may hold values from -0.125 to 0.125
- shared_down: bfloat16 [512, 2048], P('tp'), may hold values from -0.25 to 0.25
Outputs:
- layer_out: bfloat16 [2560, 2048], P(('sp', 'tp'))
The draws below stay inside these ranges and needn't reach their ends.
Inputs may be any that keep to these rules, and one draw needn't show every extreme that they name: `routes`: each row names 4 different experts; in each aligned block of 320 rows (the tokens of one index of sp) no expert is named more than 80 times, a bound that some block reaches.
All inputs are finite; a program needn't handle non-finite values.
Results may differ from the reference program's by a relative error of at most 0.019.
The reference program's roundings to bfloat16 on the way count: a program that leaves them out, or rounds other values in their place, can miss the bound.
Values may be sent and summed in bfloat16 or wider, within the bound.
A program may use at most 128 MiB of HBM per device.

```python
import math
import jax
import jax.numpy as jnp
import numpy as np
from jax import lax

D = 2048
HEAD_SIZE = 64
QUERY_HEADS = 16
KEY_VALUE_HEADS = 4
FF = 512
SFF = 512
TOPK = 4
GRID_W = 64
TOK_DEV = 320
SEQUENCE_TOKENS = 2560
EXPERTS = 32
CAP = 80
N_SP = 8
N_TP = 4


def plant_pair(key):
    unrotated_query = jnp.clip(jax.random.normal(jax.random.fold_in(key, 11), (SEQUENCE_TOKENS, QUERY_HEADS * HEAD_SIZE), jnp.float32), -6.0, 6.0)
    unrotated_key = jnp.clip(jax.random.normal(jax.random.fold_in(key, 12), (SEQUENCE_TOKENS, KEY_VALUE_HEADS * HEAD_SIZE), jnp.float32), -6.0, 6.0)
    return (unrotated_query, unrotated_key)


def draw_queries(key, part):
    return plant_pair(key)[0].astype(jnp.bfloat16)


def draw_key_matrix(key, part):
    return plant_pair(key)[1].astype(jnp.bfloat16)


def gain_draw(key, salt):
    folded = jax.random.fold_in(key, salt)
    return 1.0 + 0.18 * jnp.clip(jax.random.normal(folded, (HEAD_SIZE,), jnp.float32), -4.5, 4.5)


def draw_query_gain(key, part):
    return gain_draw(key, 21)


def draw_key_norm_gain(key, part):
    return gain_draw(key, 22)


def block_scale(key, dims, cuts, smallest, top_value):
    factor_of, own = 1.0, jax.random.fold_in(key, 6)
    for axis_at, parts in cuts:
        heights = jnp.exp(jax.random.uniform(jax.random.fold_in(own, axis_at), (parts,), jnp.float32, smallest / len(cuts), top_value / len(cuts)))
        factor_of = factor_of * jnp.repeat(heights, dims[axis_at] // parts).reshape([-1 if axis == axis_at else 1 for axis in range(len(dims))])
    return factor_of


def routed_block(own_key, own, number, rows, amount, top, limit, skew):
    order = jax.random.permutation(own_key, amount)
    packed, common = portions_of(amount, rows * top, limit, skew, True), portions_of(amount, rows * top, limit, skew, False)
    places = jnp.arange(amount)

    def named(tallies, rotation):
        used = int((tallies > 0).sum())
        fixed = max(1, used // 4)
        passed = fixed + (places - fixed + rotation * (used - fixed)) % max(1, amount - fixed)
        return jnp.zeros((amount,), jnp.int32).at[order[jnp.where(places < fixed, places, passed)]].set(jnp.asarray(tallies, jnp.int32))

    tallies = jnp.where(number % 4 == 0, named(packed, number // 4), named(common, number - number // 4 - 1))
    mixed = jax.random.permutation(jax.random.fold_in(own, 3), amount)
    source_of, receiver = mixed[0:amount // 2 * 2:2], mixed[1:amount // 2 * 2:2]
    room = jnp.minimum(tallies[source_of] - 1, limit - tallies[receiver]) // 2
    room = jnp.where((source_of == order[0]) | (receiver == order[0]) | (tallies[receiver] == 0), 0, jnp.maximum(room, 0))
    passed = jax.random.randint(jax.random.fold_in(own, 4), (amount // 2,), 0, 1 << 20) % (room + 1)
    tallies = tallies.at[source_of].add(-passed).at[receiver].add(passed)
    items = jnp.searchsorted(jnp.cumsum(tallies), jnp.arange(rows * top), side="right").astype(jnp.int32)
    grid = items.reshape(top, rows).T
    grid = grid[jax.random.permutation(jax.random.fold_in(own, 1), rows)]
    rotation = jax.random.randint(jax.random.fold_in(own, 2), (rows, 1), 0, top)
    return jnp.take_along_axis(grid, (jnp.arange(top)[None, :] + rotation) % top, axis=1)


def portions_of(number_of, total, limit, slope, full):
    weights = [(1 << 20) // math.isqrt(rank ** slope) + 1 for rank in range(1, number_of + 1)]
    largest = limit if full else min(limit, max(-(-total // number_of), total * weights[0] // sum(weights)))
    least = 1 if total - largest >= number_of - 1 else 0
    given, surplus = [largest] + [least] * (number_of - 1), total - largest - least * (number_of - 1)
    while surplus > 0:
        free = [i for i in range(1, number_of) if given[i] < largest] or [i for i in range(1, number_of) if given[i] < limit]
        whole, left = sum([weights[i] for i in free]), surplus
        for i in free:
            addition = min(limit - given[i], max(1, left * weights[i] // whole), surplus)
            given[i] = given[i] + addition
            surplus = surplus - addition
    return np.array(given)


def normal_values(rng, dims, spread, reach, cuts=(), kind=jnp.bfloat16):
    values = spread * jax.random.normal(rng, dims, jnp.float32)
    if cuts:
        values = values * block_scale(rng, dims, cuts, -0.22, 0.18)
    return jnp.clip(values, -reach, reach).astype(kind)


def setup_inputs(seed: int = 0) -> dict:
    seeds = jax.random.split(jax.random.key(seed), 18)
    queries = draw_queries(jax.random.fold_in(seeds[17], 71), 0)
    key_matrix = draw_key_matrix(jax.random.fold_in(seeds[17], 71), 0)
    values = normal_values(seeds[2], (SEQUENCE_TOKENS, KEY_VALUE_HEADS * HEAD_SIZE), 1.0, 6.0, ((0, 8), (1, 4)))
    query_gain = draw_query_gain(jax.random.fold_in(seeds[17], 71), 0)
    key_norm_gain = draw_key_norm_gain(jax.random.fold_in(seeds[17], 71), 0)
    head_gain = jnp.clip(1.0 + 0.18 * jax.random.normal(seeds[5], (QUERY_HEADS * HEAD_SIZE,), jnp.float32), 0.1, 1.9)
    out_proj = normal_values(seeds[6], (QUERY_HEADS * HEAD_SIZE, D), (QUERY_HEADS * HEAD_SIZE) ** -0.5, 0.1875)
    residual = normal_values(seeds[7], (SEQUENCE_TOKENS, D), 1.0, 6.0, ((0, 8),))
    ffn_gain = jnp.clip(1.0 + 0.18 * jax.random.normal(seeds[8], (D,), jnp.float32), 0.1, 1.9)
    routes_keys = jax.random.split(jax.random.fold_in(seeds[9], 1), SEQUENCE_TOKENS // TOK_DEV)
    routes_turns = jax.random.permutation(jax.random.fold_in(seeds[9], 3), SEQUENCE_TOKENS // TOK_DEV)
    routes = jax.vmap(lambda own, number: routed_block(jax.random.fold_in(seeds[9], 2), own, number, TOK_DEV, EXPERTS, TOPK, CAP, 1))(routes_keys, routes_turns).reshape((SEQUENCE_TOKENS, TOPK))
    route_weights = jnp.clip(0.2 + 0.8 * jax.random.uniform(seeds[10], (SEQUENCE_TOKENS, TOPK), jnp.float32) ** block_scale(seeds[10], (SEQUENCE_TOKENS, TOPK), ((0, 8),), -0.2, 0.2), 0.2, 1.0)
    expert_gate = normal_values(seeds[11], (EXPERTS, D, FF), D ** -0.5, 0.125, ((0, 32),))
    expert_up = normal_values(seeds[12], (EXPERTS, D, FF), D ** -0.5, 0.125, ((0, 32),))
    expert_down = normal_values(seeds[13], (EXPERTS, FF, D), FF ** -0.5, 0.25, ((0, 32),))
    shared_gate = normal_values(seeds[14], (D, SFF), D ** -0.5, 0.125, ((1, 4),))
    shared_up = normal_values(seeds[15], (D, SFF), D ** -0.5, 0.125, ((1, 4),))
    shared_down = normal_values(seeds[16], (SFF, D), SFF ** -0.5, 0.25, ((0, 4),))
    return dict(queries=queries, key_matrix=key_matrix, values=values, query_gain=query_gain, key_norm_gain=key_norm_gain, head_gain=head_gain, out_proj=out_proj, residual=residual, ffn_gain=ffn_gain, routes=routes, route_weights=route_weights, expert_gate=expert_gate, expert_up=expert_up, expert_down=expert_down, shared_gate=shared_gate, shared_up=shared_up, shared_down=shared_down)


EPS = 1e-06
THETA = 10000.0

def final_norm(field, gain):
    mean_sq = lax.optimization_barrier(jnp.mean(field * field, axis=-1, keepdims=True))
    return field * lax.rsqrt(mean_sq + EPS) * gain

def grid_tables(positions, sequence_total):
    grid_rows = sequence_total // GRID_W
    row_pos = (positions // GRID_W - grid_rows // 2).astype(jnp.float32)
    col_pos = (positions % GRID_W - GRID_W // 2).astype(jnp.float32)
    quarter = HEAD_SIZE // 4
    inverse = THETA ** (-jnp.arange(quarter, dtype=jnp.float32) / quarter)
    angles = jnp.concatenate([row_pos[:, None] * inverse, col_pos[:, None] * inverse], axis=1)
    return (jnp.cos(angles), jnp.sin(angles))

def apply_rotary(field, cosine_table, sine_table):
    row_count, head_count = (field.shape[0], field.shape[1])
    quarter = HEAD_SIZE // 4
    pieces = field.reshape(row_count, head_count, 2, 2, quarter)
    front_half = pieces[:, :, :, 0, :].reshape(row_count, head_count, 2 * quarter)
    back_half = pieces[:, :, :, 1, :].reshape(row_count, head_count, 2 * quarter)
    cos_wide = cosine_table[:, None, :]
    sin_wide = sine_table[:, None, :]
    new_front = (front_half * cos_wide - back_half * sin_wide).reshape(row_count, head_count, 2, 1, quarter)
    new_back = (front_half * sin_wide + back_half * cos_wide).reshape(row_count, head_count, 2, 1, quarter)
    return jnp.concatenate([new_front, new_back], axis=3).reshape(row_count, head_count, HEAD_SIZE)

def reference(queries, key_matrix, values, query_gain, key_norm_gain, head_gain, out_proj, residual, ffn_gain, routes, route_weights, expert_gate, expert_up, expert_down, shared_gate, shared_up, shared_down):
    sequence_total = SEQUENCE_TOKENS
    positions = jnp.arange(sequence_total, dtype=jnp.int32)
    cosine_table, sine_table = grid_tables(positions, sequence_total)
    rotated_query = apply_rotary(final_norm(queries.astype(jnp.float32).reshape(sequence_total, QUERY_HEADS, HEAD_SIZE), query_gain), cosine_table, sine_table).astype(jnp.bfloat16)
    rotated_key = apply_rotary(final_norm(key_matrix.astype(jnp.float32).reshape(sequence_total, KEY_VALUE_HEADS, HEAD_SIZE), key_norm_gain), cosine_table, sine_table).astype(jnp.bfloat16)
    group_width = QUERY_HEADS // KEY_VALUE_HEADS
    block_length = 64
    query_block_list = rotated_query.reshape(sequence_total // block_length, block_length, KEY_VALUE_HEADS, group_width, HEAD_SIZE)
    key_wide = rotated_key.astype(jnp.float32)
    value_expanded = values.reshape(sequence_total, KEY_VALUE_HEADS, HEAD_SIZE).astype(jnp.float32)
    score_scale = HEAD_SIZE ** (-0.5)

    def attend(query_block):
        scores = jnp.einsum('qkgd,skd->kgqs', query_block.astype(jnp.float32), key_wide) * score_scale
        row_max = lax.optimization_barrier(jnp.max(scores, axis=-1, keepdims=True))
        expo_terms = jnp.exp(scores - row_max)
        weights = lax.optimization_barrier(expo_terms.astype(jnp.bfloat16)).astype(jnp.float32)
        mixed_vals = jnp.einsum('kgqs,skd->qkgd', weights, value_expanded)
        denominator = jnp.moveaxis(lax.optimization_barrier(jnp.sum(expo_terms, axis=-1)), -1, 0)
        return mixed_vals / denominator[..., None]
    attended = lax.map(attend, query_block_list).reshape(sequence_total, QUERY_HEADS, HEAD_SIZE)
    head_out = final_norm(attended, head_gain.reshape(QUERY_HEADS, HEAD_SIZE)).astype(jnp.bfloat16).reshape(sequence_total, QUERY_HEADS * HEAD_SIZE)
    hidden = (residual.astype(jnp.float32) + jnp.dot(head_out, out_proj, preferred_element_type=jnp.float32)).astype(jnp.bfloat16)
    normed = final_norm(hidden.astype(jnp.float32), ffn_gain).astype(jnp.bfloat16)
    flat_expert = routes.reshape(-1).astype(jnp.int32)
    entries = flat_expert.shape[0]
    order_ids = jnp.argsort(flat_expert, stable=True).astype(jnp.int32)
    sorted_expert = flat_expert[order_ids]
    counts_per = jnp.bincount(flat_expert, length=EXPERTS).astype(jnp.int32)
    starts = (jnp.cumsum(counts_per) - counts_per).astype(jnp.int32)
    rank_ids = (jnp.arange(entries, dtype=jnp.int32) - starts[sorted_expert]).astype(jnp.int32)
    slot_table = jnp.full((EXPERTS, N_SP * CAP), entries, jnp.int32).at[sorted_expert, rank_ids].set(order_ids)
    entry_weight = jnp.concatenate([route_weights.reshape(-1), jnp.zeros((1,), jnp.float32)])
    entry_token = jnp.concatenate([jnp.arange(entries, dtype=jnp.int32) // TOPK, jnp.zeros((1,), jnp.int32)])
    slice_width = SFF // N_TP
    result = hidden.astype(jnp.float32)
    for owner in range(N_TP):
        col_start = owner * slice_width
        gate_part = jnp.dot(normed, shared_gate[:, col_start:col_start + slice_width], preferred_element_type=jnp.float32)
        up_part = jnp.dot(normed, shared_up[:, col_start:col_start + slice_width], preferred_element_type=jnp.float32)
        inner_act = (jax.nn.silu(gate_part) * up_part).astype(jnp.bfloat16)
        partial_sum = jnp.dot(inner_act, shared_down[col_start:col_start + slice_width, :], preferred_element_type=jnp.float32)

        def add_expert(total_acc, local_index, owner=owner):
            expert = local_index * N_TP + owner
            entry_ids = slot_table[expert]
            token_ids = entry_token[entry_ids]
            rows_in = normed[token_ids]
            gate_out = jnp.dot(rows_in, expert_gate[expert], preferred_element_type=jnp.float32)
            up_out = jnp.dot(rows_in, expert_up[expert], preferred_element_type=jnp.float32)
            expert_inner = (jax.nn.silu(gate_out) * up_out).astype(jnp.bfloat16)
            produced = jnp.dot(expert_inner, expert_down[expert], preferred_element_type=jnp.float32).astype(jnp.bfloat16)
            weighted = produced.astype(jnp.float32) * entry_weight[entry_ids][:, None]
            return (total_acc.at[token_ids].add(weighted), None)
        partial_sum, _ = lax.scan(add_expert, partial_sum, jnp.arange(EXPERTS // N_TP, dtype=jnp.int32))
        result = result + lax.optimization_barrier(partial_sum.astype(jnp.bfloat16)).astype(jnp.float32)
    return result.astype(jnp.bfloat16)
```

```python
import jax
import jax.numpy as jnp
from jax import lax
from jax.experimental import pallas as pl
from jax.experimental.pallas import tpu as pltpu
from jax.sharding import PartitionSpec as P

HEAD_SIZE = 64
GRID_W = 64


EPS = 1e-06
THETA = 10000.0


def final_norm(field, gain):
    mean_sq = jnp.mean(field * field, axis=-1, keepdims=True)
    return field * lax.rsqrt(mean_sq + EPS) * gain


def grid_tables(positions, sequence_total):
    grid_rows = sequence_total // GRID_W
    row_pos = (positions // GRID_W - grid_rows // 2).astype(jnp.float32)
    col_pos = (positions % GRID_W - GRID_W // 2).astype(jnp.float32)
    quarter = HEAD_SIZE // 4
    inverse = THETA ** (-jnp.arange(quarter, dtype=jnp.float32) / quarter)
    angles = jnp.concatenate([row_pos[:, None] * inverse, col_pos[:, None] * inverse], axis=1)
    return (jnp.cos(angles), jnp.sin(angles))


def apply_rotary(field, cosine_table, sine_table):
    row_count, head_count = (field.shape[0], field.shape[1])
    quarter = HEAD_SIZE // 4
    pieces = field.reshape(row_count, head_count, 2, 2, quarter)
    front_half = pieces[:, :, :, 0, :].reshape(row_count, head_count, 2 * quarter)
    back_half = pieces[:, :, :, 1, :].reshape(row_count, head_count, 2 * quarter)
    cos_wide = cosine_table[:, None, :]
    sin_wide = sine_table[:, None, :]
    new_front = (front_half * cos_wide - back_half * sin_wide).reshape(
        row_count, head_count, 2, 1, quarter
    )
    new_back = (front_half * sin_wide + back_half * cos_wide).reshape(
        row_count, head_count, 2, 1, quarter
    )
    return jnp.concatenate([new_front, new_back], axis=3).reshape(row_count, head_count, HEAD_SIZE)


def exchange(block, axis, call_id, gather):
    count = lax.axis_size(axis)
    if count == 1:
        return block[None] if gather else block
    shape = (count,) + block.shape if gather else block.shape

    def kernel(in_ref, out_ref, send_sems, recv_sems, own_sem):
        me = lax.axis_index(axis)
        barrier = pltpu.get_barrier_semaphore()
        for step in range(1, count):
            pl.semaphore_signal(
                barrier,
                inc=1,
                device_id={axis: lax.rem(me + step, count)},
                device_id_type=pl.DeviceIdType.MESH,
            )
        own = pltpu.make_async_copy(in_ref if gather else in_ref.at[me], out_ref.at[me], own_sem)
        own.start()
        pl.semaphore_wait(barrier, count - 1)
        copies = []
        for step in range(1, count):
            peer = lax.rem(me + step, count)
            copy = pltpu.make_async_remote_copy(
                src_ref=in_ref if gather else in_ref.at[peer],
                dst_ref=out_ref.at[me],
                send_sem=send_sems.at[step],
                recv_sem=recv_sems.at[step],
                device_id={axis: peer},
                device_id_type=pl.DeviceIdType.MESH,
            )
            copy.start()
            copies.append(copy)
        own.wait()
        for copy in copies:
            copy.wait()

    return pl.pallas_call(
        kernel,
        out_shape=jax.ShapeDtypeStruct(shape, block.dtype),
        in_specs=[pl.BlockSpec(memory_space=pltpu.VMEM)],
        out_specs=pl.BlockSpec(memory_space=pltpu.VMEM),
        scratch_shapes=[
            pltpu.SemaphoreType.DMA((count,)),
            pltpu.SemaphoreType.DMA((count,)),
            pltpu.SemaphoreType.DMA,
        ],
        compiler_params=pltpu.CompilerParams(collective_id=call_id, has_side_effects=True),
        name="exchange_%d" % call_id,
    )(block)


def key_block_rows(piece_rows):
    return max((width for width in range(1, 2049) if piece_rows % width == 0))


def local(
    queries,
    key_matrix,
    values,
    query_gain,
    key_norm_gain,
    head_gain,
    out_proj,
    residual,
    ffn_gain,
    routes,
    route_weights,
    expert_gate,
    expert_up,
    expert_down,
    shared_gate,
    shared_up,
    shared_down,
):
    tok_count = queries.shape[0]
    head_count = queries.shape[1] // HEAD_SIZE
    sp_count = lax.axis_size("sp")
    tp_count = lax.axis_size("tp")
    tp_index = lax.axis_index("tp")
    sequence_total = tok_count * sp_count
    positions = lax.axis_index("sp") * tok_count + jnp.arange(tok_count, dtype=jnp.int32)
    cosine_table, sine_table = grid_tables(positions, sequence_total)
    rotated_query = apply_rotary(
        final_norm(
            queries.astype(jnp.float32).reshape(tok_count, head_count, HEAD_SIZE), query_gain
        ),
        cosine_table,
        sine_table,
    ).astype(jnp.bfloat16)
    rotated_key = (
        apply_rotary(
            final_norm(
                key_matrix.astype(jnp.float32).reshape(tok_count, 1, HEAD_SIZE), key_norm_gain
            ),
            cosine_table,
            sine_table,
        )
        .reshape(tok_count, HEAD_SIZE)
        .astype(jnp.bfloat16)
    )
    packed = jnp.concatenate([rotated_key, values], axis=1)
    query_rows = rotated_query.transpose(1, 0, 2).reshape(head_count * tok_count, HEAD_SIZE)
    score_scale = HEAD_SIZE ** (-0.5)
    start_state = (
        jnp.full((head_count * tok_count,), -1e30, jnp.float32),
        jnp.zeros((head_count * tok_count,), jnp.float32),
        jnp.zeros((head_count * tok_count, HEAD_SIZE), jnp.float32),
    )
    state = start_state
    piece = exchange(packed, "sp", 0, True).reshape(sequence_total, 2 * HEAD_SIZE)
    piece_rows = piece.shape[0]
    block_length = key_block_rows(piece_rows)
    key_blocks = piece.reshape(piece_rows // block_length, block_length, 2 * HEAD_SIZE)

    def step(carry, key_slab):
        run_max, run_total, run_acc = carry
        scores = (
            lax.dot_general(
                query_rows,
                key_slab[:, :HEAD_SIZE],
                (((1,), (1,)), ((), ())),
                preferred_element_type=jnp.float32,
            )
            * score_scale
        )
        new_max = jnp.maximum(run_max, jnp.max(scores, axis=1))
        factor = jnp.exp(run_max - new_max)
        expo_terms = jnp.exp(scores - new_max[:, None])
        new_total = run_total * factor + jnp.sum(expo_terms, axis=1)
        new_acc = run_acc * factor[:, None] + jnp.dot(
            expo_terms.astype(jnp.bfloat16),
            key_slab[:, HEAD_SIZE:],
            preferred_element_type=jnp.float32,
        )
        return ((new_max, new_total, new_acc), None)

    state, _ = lax.scan(step, state, key_blocks)
    run_max, run_total, run_acc = state
    attended = (
        (run_acc / run_total[:, None]).reshape(head_count, tok_count, HEAD_SIZE).transpose(1, 0, 2)
    )
    head_out = final_norm(attended, head_gain.reshape(head_count, HEAD_SIZE)).astype(jnp.bfloat16)
    head_out = head_out.reshape(tok_count, head_count * HEAD_SIZE)
    part_rows = tok_count // tp_count
    token_heads = exchange(
        head_out.reshape(tp_count, part_rows, head_count * HEAD_SIZE), "tp", 1, False
    )
    token_heads = token_heads.transpose(1, 0, 2).reshape(part_rows, -1)
    own_resid = lax.dynamic_slice_in_dim(residual, tp_index * part_rows, part_rows, 0)
    hidden_own = (
        own_resid.astype(jnp.float32)
        + jnp.dot(token_heads, out_proj, preferred_element_type=jnp.float32)
    ).astype(jnp.bfloat16)
    normed_own = final_norm(hidden_own.astype(jnp.float32), ffn_gain).astype(jnp.bfloat16)
    model_width = normed_own.shape[1]
    normed = exchange(normed_own, "tp", 2, True).reshape(tok_count, model_width)
    topk_count = routes.shape[1]
    capacity = max(2, 2 * tok_count * topk_count // (sp_count * tp_count))
    slot_total = sp_count * capacity
    experts_here = jnp.arange(sp_count, dtype=jnp.int32) * tp_count + tp_index
    named = routes[:, :, None] == experts_here[None, None, :]
    member = jnp.any(named, axis=1)
    scale = jnp.sum(jnp.where(named, route_weights[:, :, None], 0.0), axis=1)
    order = jnp.arange(tok_count, dtype=jnp.int32)
    before = (order[:, None] > order[None, :]).astype(jnp.bfloat16)
    rank = jnp.dot(
        before, member.astype(jnp.bfloat16), preferred_element_type=jnp.float32
    ).astype(jnp.int32)
    rank = jnp.where(member, rank, -1)
    slots = jnp.arange(capacity, dtype=jnp.int32)
    chosen = rank.T[:, None, :] == slots[None, :, None]
    select = chosen.astype(jnp.bfloat16).reshape(slot_total, tok_count)
    outgoing = jnp.dot(select, normed, preferred_element_type=jnp.float32).astype(jnp.bfloat16)
    gate_local = expert_gate[0]
    up_local = expert_up[0]
    down_local = expert_down[0]
    arrived = exchange(outgoing.reshape(sp_count, capacity, model_width), "sp", 3, False)
    flat_rows = arrived.reshape(slot_total, model_width)
    gate_out = jnp.dot(flat_rows, gate_local, preferred_element_type=jnp.float32)
    up_out = jnp.dot(flat_rows, up_local, preferred_element_type=jnp.float32)
    expert_inner = (jax.nn.silu(gate_out) * up_out).astype(jnp.bfloat16)
    produced = jnp.dot(expert_inner, down_local, preferred_element_type=jnp.float32).astype(
        jnp.bfloat16
    )
    returned = exchange(produced.reshape(sp_count, capacity, model_width), "sp", 4, False).reshape(
        slot_total, model_width
    )
    combine = jnp.where(chosen, scale.T[:, None, :], 0.0).reshape(slot_total, tok_count)
    combine_hi = lax.reduce_precision(combine, 8, 7)
    combine_lo = (combine - combine_hi).astype(jnp.bfloat16)
    combine_hi = combine_hi.astype(jnp.bfloat16)

    def mix(weights):
        return lax.dot_general(
            weights, returned, (((0,), (0,)), ((), ())), preferred_element_type=jnp.float32
        )

    gate_part = jnp.dot(normed, shared_gate, preferred_element_type=jnp.float32)
    up_part = jnp.dot(normed, shared_up, preferred_element_type=jnp.float32)
    shared_inner = (jax.nn.silu(gate_part) * up_part).astype(jnp.bfloat16)
    shares = (
        jnp.dot(shared_inner, shared_down, preferred_element_type=jnp.float32)
        + mix(combine_hi)
        + mix(combine_lo)
    ).astype(jnp.bfloat16)
    shares = exchange(shares.reshape(tp_count, part_rows, model_width), "tp", 5, False)
    mixed_rows = jnp.sum(shares.astype(jnp.float32), axis=0)
    return (hidden_own.astype(jnp.float32) + mixed_rows).astype(jnp.bfloat16)


def solution(mesh):
    placed = (
        P("sp", "tp"),
        P("sp", "tp"),
        P("sp", "tp"),
        P(),
        P(),
        P("tp"),
        P(),
        P("sp", None),
        P(),
        P("sp", None),
        P("sp", None),
        P(("sp", "tp"), None, None),
        P(("sp", "tp"), None, None),
        P(("sp", "tp"), None, None),
        P(None, "tp"),
        P(None, "tp"),
        P("tp", None),
    )
    return jax.shard_map(
        local, mesh=mesh, in_specs=placed, out_specs=P(("sp", "tp"), None), check_vma=False
    )
```

```python
import jax
import jax.numpy as jnp
from jax import lax
from jax.experimental import pallas as pl
from jax.experimental.pallas import tpu as pltpu
from jax.sharding import PartitionSpec as P

HEAD_SIZE = 64
GRID_W = 64


EPS = 1e-06
THETA = 10000.0


def final_norm(field, gain):
    mean_sq = jnp.mean(field * field, axis=-1, keepdims=True)
    return field * lax.rsqrt(mean_sq + EPS) * gain


def grid_tables(positions, sequence_total):
    grid_rows = sequence_total // GRID_W
    row_pos = (positions // GRID_W - grid_rows // 2).astype(jnp.float32)
    col_pos = (positions % GRID_W - GRID_W // 2).astype(jnp.float32)
    quarter = HEAD_SIZE // 4
    inverse = THETA ** (-jnp.arange(quarter, dtype=jnp.float32) / quarter)
    angles = jnp.concatenate([row_pos[:, None] * inverse, col_pos[:, None] * inverse], axis=1)
    return (jnp.cos(angles), jnp.sin(angles))


def apply_rotary(field, cosine_table, sine_table):
    row_count, head_count = (field.shape[0], field.shape[1])
    quarter = HEAD_SIZE // 4
    pieces = field.reshape(row_count, head_count, 2, 2, quarter)
    front_half = pieces[:, :, :, 0, :].reshape(row_count, head_count, 2 * quarter)
    back_half = pieces[:, :, :, 1, :].reshape(row_count, head_count, 2 * quarter)
    cos_wide = cosine_table[:, None, :]
    sin_wide = sine_table[:, None, :]
    new_front = (front_half * cos_wide - back_half * sin_wide).reshape(
        row_count, head_count, 2, 1, quarter
    )
    new_back = (front_half * sin_wide + back_half * cos_wide).reshape(
        row_count, head_count, 2, 1, quarter
    )
    return jnp.concatenate([new_front, new_back], axis=3).reshape(row_count, head_count, HEAD_SIZE)


def exchange(block, axis, call_id, gather):
    count = lax.axis_size(axis)
    if count == 1:
        return block[None] if gather else block
    shape = (count,) + block.shape if gather else block.shape

    def kernel(in_ref, out_ref, send_sems, recv_sems, own_sem):
        me = lax.axis_index(axis)
        barrier = pltpu.get_barrier_semaphore()
        for step in range(1, count):
            pl.semaphore_signal(
                barrier,
                inc=1,
                device_id={axis: lax.rem(me + step, count)},
                device_id_type=pl.DeviceIdType.MESH,
            )
        own = pltpu.make_async_copy(in_ref if gather else in_ref.at[me], out_ref.at[me], own_sem)
        own.start()
        pl.semaphore_wait(barrier, count - 1)
        copies = []
        for step in range(1, count):
            peer = lax.rem(me + step, count)
            copy = pltpu.make_async_remote_copy(
                src_ref=in_ref if gather else in_ref.at[peer],
                dst_ref=out_ref.at[me],
                send_sem=send_sems.at[step],
                recv_sem=recv_sems.at[step],
                device_id={axis: peer},
                device_id_type=pl.DeviceIdType.MESH,
            )
            copy.start()
            copies.append(copy)
        own.wait()
        for copy in copies:
            copy.wait()

    return pl.pallas_call(
        kernel,
        out_shape=jax.ShapeDtypeStruct(shape, block.dtype),
        in_specs=[pl.BlockSpec(memory_space=pltpu.VMEM)],
        out_specs=pl.BlockSpec(memory_space=pltpu.VMEM),
        scratch_shapes=[
            pltpu.SemaphoreType.DMA((count,)),
            pltpu.SemaphoreType.DMA((count,)),
            pltpu.SemaphoreType.DMA,
        ],
        compiler_params=pltpu.CompilerParams(collective_id=call_id, has_side_effects=True),
        name="exchange_%d" % call_id,
    )(block)


def key_block_rows(piece_rows):
    return max((width for width in range(1, 2049) if piece_rows % width == 0))


MESH = pl.DeviceIdType.MESH
COLUMNS = 512


def proxy_plane(t):
    pair, side = t // 2, t % 2
    return pair + side * (3 - 2 * pair)


def proxy_of(plane):
    return jnp.where(plane == 0, 0, jnp.where(plane == 3, 1, plane + 1))


def place(planes, width, tp_count):
    sp, t = lax.axis_index("sp"), lax.axis_index("tp")
    z, x = sp // width, sp % width
    return z, x, t, x * tp_count + t


def greet(z, x, p, planes, width, tp_count):
    barrier = pltpu.get_barrier_semaphore()
    group = width * tp_count
    for step in range(1, group):
        peer = lax.rem(p + step, group)
        pl.semaphore_signal(
            barrier,
            inc=1,
            device_id={"sp": z * width + peer // tp_count, "tp": peer % tp_count},
            device_id_type=MESH,
        )
    for step in (1, planes - 1):
        pl.semaphore_signal(
            barrier,
            inc=1,
            device_id={"sp": lax.rem(z + step, planes) * width + x},
            device_id_type=MESH,
        )
    pl.semaphore_wait(barrier, group - 1 + 2)


def dispatch(normed_own, select, planes, width, tp_count, call_id):
    rows, model = normed_own.shape
    group, capacity, tokens = select.shape
    quarters = tokens // rows

    def kernel(own_ref, sel_ref, out_ref, blk, packed, a_send, z_send, b_recv, c_send, c_recv, sem):
        z, x, t, p = place(planes, width, tp_count)
        zb = proxy_plane(t)
        home = z == zb
        greet(z, x, p, planes, width, tp_count)
        target = proxy_of(z)

        def to_home():
            return pltpu.make_async_remote_copy(
                src_ref=own_ref,
                dst_ref=blk.at[t],
                send_sem=a_send,
                recv_sem=b_recv.at[t],
                device_id={"tp": target},
                device_id_type=MESH,
            )

        @pl.when(t != target)
        def _():
            to_home().start()

        own_copy = pltpu.make_async_copy(own_ref, blk.at[t], sem)

        @pl.when(home)
        def _():
            own_copy.start()
            own_copy.wait()

        def relay(q, up):
            return pltpu.make_async_remote_copy(
                src_ref=blk.at[q],
                dst_ref=blk.at[q],
                send_sem=z_send.at[up, q],
                recv_sem=b_recv.at[q],
                device_id={"sp": (z + (1 if up else -1)) * width + x},
                device_id_type=MESH,
            )

        go_up = (z >= zb) & (z < planes - 1)
        go_down = (z <= zb) & (z > 0)

        for k in range(quarters):
            q = lax.rem(t + k, quarters)

            @pl.when(jnp.logical_not(home & (q == t)))
            def _():
                relay(q, 1).wait_recv()

            @pl.when(go_up)
            def _():
                relay(q, 1).start()

            @pl.when(go_down)
            def _():
                relay(q, 0).start()

        def send(pp):
            return pltpu.make_async_remote_copy(
                src_ref=packed.at[pp],
                dst_ref=out_ref.at[zb * width + x],
                send_sem=c_send.at[pp],
                recv_sem=c_recv.at[zb * width + x],
                device_id={"sp": z * width + pp // tp_count, "tp": pp % tp_count},
                device_id_type=MESH,
            )

        def serve(k, carry):
            pp = lax.rem(p + 1 + k, group)
            chosen = sel_ref[pp]
            for column in range(0, model, COLUMNS):
                part = pl.ds(column, COLUMNS)
                packed[pp, :, part] = jnp.dot(
                    chosen,
                    blk[:, :, part].reshape(tokens, COLUMNS),
                    preferred_element_type=jnp.float32,
                ).astype(jnp.bfloat16)

            @pl.when(pp != p)
            def _():
                send(pp).start()

            return carry

        lax.fori_loop(0, group, serve, 0)
        kept = pltpu.make_async_copy(packed.at[p], out_ref.at[zb * width + x], sem)
        kept.start()
        kept.wait()

        def finish(k, carry):
            pp = lax.rem(p + 1 + k, group)
            send(pp).wait_send()
            source = proxy_plane(pp % tp_count) * width + pp // tp_count
            pltpu.make_async_remote_copy(
                src_ref=packed.at[pp],
                dst_ref=out_ref.at[source],
                send_sem=c_send.at[pp],
                recv_sem=c_recv.at[source],
                device_id={"sp": z * width + pp // tp_count, "tp": pp % tp_count},
                device_id_type=MESH,
            ).wait_recv()
            return carry

        lax.fori_loop(0, group - 1, finish, 0)

        @pl.when(t != target)
        def _():
            to_home().wait_send()

        for q in range(quarters):

            @pl.when(go_up)
            def _():
                relay(q, 1).wait_send()

            @pl.when(go_down)
            def _():
                relay(q, 0).wait_send()

    vmem = pl.BlockSpec(memory_space=pltpu.VMEM)
    dma = pltpu.SemaphoreType.DMA
    return pl.pallas_call(
        kernel,
        out_shape=jax.ShapeDtypeStruct((planes * width, capacity, model), jnp.bfloat16),
        in_specs=[vmem] * 2,
        out_specs=vmem,
        scratch_shapes=[
            pltpu.VMEM((quarters, rows, model), jnp.bfloat16),
            pltpu.VMEM((group, capacity, model), jnp.bfloat16),
            dma,
            dma((2, quarters)),
            dma((quarters,)),
            dma((group,)),
            dma((planes * width,)),
            dma,
        ],
        compiler_params=pltpu.CompilerParams(collective_id=call_id, has_side_effects=True),
        name="dispatch",
    )(normed_own, select)


def give_back(produced, weights_hi, weights_lo, planes, width, tp_count, call_id):
    blocks, capacity, model = produced.shape
    quarters, rows, slots = weights_hi.shape
    group = width * tp_count

    def kernel(
        in_ref, hi_ref, lo_ref, out_ref,
        back, total, passed, arrived, c_send, c_recv, z_send, z_recv, a_recv, sem,
    ):
        z, x, t, p = place(planes, width, tp_count)
        zb = proxy_plane(t)
        home = z == zb
        greet(z, x, p, planes, width, tp_count)
        keep = pltpu.make_async_copy(in_ref.at[zb * width + x], back.at[p], sem)
        keep.start()

        def send(pp):
            return pltpu.make_async_remote_copy(
                src_ref=in_ref.at[proxy_plane(pp % tp_count) * width + pp // tp_count],
                dst_ref=back.at[p],
                send_sem=c_send.at[pp],
                recv_sem=c_recv.at[p],
                device_id={"sp": z * width + pp // tp_count, "tp": pp % tp_count},
                device_id_type=MESH,
            )

        def came(pp):
            return pltpu.make_async_remote_copy(
                src_ref=in_ref.at[0],
                dst_ref=back.at[pp],
                send_sem=c_send.at[pp],
                recv_sem=c_recv.at[pp],
                device_id={"sp": z * width + pp // tp_count, "tp": pp % tp_count},
                device_id_type=MESH,
            )

        def issue(k, carry):
            rank = k // width
            plane = jnp.where(2 * z < planes, planes - 1 - rank, rank)
            pp = lax.rem(x + k + 1, width) * tp_count + proxy_of(plane)

            @pl.when(pp != p)
            def _():
                send(pp).start()

            return carry

        lax.fori_loop(0, group, issue, 0)
        keep.wait()

        def collect(k, carry):
            came(lax.rem(p + 1 + k, group)).wait_recv()
            return carry

        lax.fori_loop(0, group - 1, collect, 0)

        from_above = (z >= zb) & (z < planes - 1)
        from_below = (z <= zb) & (z > 0)

        def hop(q, down):
            return pltpu.make_async_remote_copy(
                src_ref=passed.at[q],
                dst_ref=arrived.at[down, q],
                send_sem=z_send.at[q],
                recv_sem=z_recv.at[down, q],
                device_id={"sp": (z + (-1 if down else 1)) * width + x},
                device_id_type=MESH,
            )

        def to_owner(q):
            return pltpu.make_async_remote_copy(
                src_ref=passed.at[q],
                dst_ref=out_ref,
                send_sem=z_send.at[q],
                recv_sem=a_recv,
                device_id={"tp": q},
                device_id_type=MESH,
            )

        def quarter(q, carry):
            for column in range(0, model, COLUMNS):
                part = pl.ds(column, COLUMNS)
                piece = back[:, :, part].reshape(slots, COLUMNS)
                total[:, part] = jnp.dot(
                    hi_ref[q], piece, preferred_element_type=jnp.float32
                ) + jnp.dot(lo_ref[q], piece, preferred_element_type=jnp.float32)

            @pl.when(from_above)
            def _():
                hop(q, 1).wait_recv()
                total[...] += arrived[1, q].astype(jnp.float32)

            @pl.when(from_below)
            def _():
                hop(q, 0).wait_recv()
                total[...] += arrived[0, q].astype(jnp.float32)

            passed[q] = total[...].astype(jnp.bfloat16)

            @pl.when(z > zb)
            def _():
                hop(q, 1).start()

            @pl.when(z < zb)
            def _():
                hop(q, 0).start()

            @pl.when(home & (q != t))
            def _():
                to_owner(q).start()

            @pl.when(home & (q == t))
            def _():
                mine = pltpu.make_async_copy(passed.at[q], out_ref, sem)
                mine.start()
                mine.wait()

            return carry

        lax.fori_loop(0, quarters, quarter, 0)

        @pl.when(jnp.logical_not(home))
        def _():
            to_owner(t).wait_recv()

        def sent(k, carry):
            send(lax.rem(p + 1 + k, group)).wait_send()
            return carry

        lax.fori_loop(0, group - 1, sent, 0)

        def left(q, carry):
            @pl.when(jnp.logical_not(home & (q == t)))
            def _():
                to_owner(q).wait_send()

            return carry

        lax.fori_loop(0, quarters, left, 0)

    vmem = pl.BlockSpec(memory_space=pltpu.VMEM)
    dma = pltpu.SemaphoreType.DMA
    return pl.pallas_call(
        kernel,
        out_shape=jax.ShapeDtypeStruct((rows, model), jnp.bfloat16),
        in_specs=[vmem] * 3,
        out_specs=vmem,
        scratch_shapes=[
            pltpu.VMEM((group, capacity, model), jnp.bfloat16),
            pltpu.VMEM((rows, model), jnp.float32),
            pltpu.VMEM((quarters, rows, model), jnp.bfloat16),
            pltpu.VMEM((2, quarters, rows, model), jnp.bfloat16),
            dma((group,)),
            dma((group,)),
            dma((quarters,)),
            dma((2, quarters)),
            dma,
            dma,
        ],
        compiler_params=pltpu.CompilerParams(collective_id=call_id, has_side_effects=True),
        name="give_back",
    )(produced, weights_hi, weights_lo)


def spread_shards(shard, tp_count):
    across = lax.ppermute(shard, "tp", [(i, i ^ 2) for i in range(tp_count)])
    beside = [(i, i ^ 1) for i in range(tp_count)]
    return [shard, across, lax.ppermute(shard, "tp", beside), lax.ppermute(across, "tp", beside)]


def slot_ranks(member):
    order = jnp.arange(member.shape[0], dtype=jnp.int32)
    before = (order[:, None] > order[None, :]).astype(jnp.bfloat16)
    rank = jnp.dot(before, member.astype(jnp.bfloat16), preferred_element_type=jnp.float32)
    return jnp.where(member, rank.astype(jnp.int32), -1)


def expert_block(flat_rows, gate_local, up_local, down_local):
    gate_out = jnp.dot(flat_rows, gate_local, preferred_element_type=jnp.float32)
    up_out = jnp.dot(flat_rows, up_local, preferred_element_type=jnp.float32)
    expert_inner = (jax.nn.silu(gate_out) * up_out).astype(jnp.bfloat16)
    return jnp.dot(expert_inner, down_local, preferred_element_type=jnp.float32).astype(
        jnp.bfloat16
    )


def local(
    queries,
    key_matrix,
    values,
    query_gain,
    key_norm_gain,
    head_gain,
    out_proj,
    residual,
    ffn_gain,
    routes,
    route_weights,
    expert_gate,
    expert_up,
    expert_down,
    shared_gate,
    shared_up,
    shared_down,
):
    tok_count = queries.shape[0]
    head_count = queries.shape[1] // HEAD_SIZE
    sp_count = lax.axis_size("sp")
    tp_count = lax.axis_size("tp")
    tp_index = lax.axis_index("tp")
    sequence_total = tok_count * sp_count
    positions = lax.axis_index("sp") * tok_count + jnp.arange(tok_count, dtype=jnp.int32)
    cosine_table, sine_table = grid_tables(positions, sequence_total)
    rotated_query = apply_rotary(
        final_norm(
            queries.astype(jnp.float32).reshape(tok_count, head_count, HEAD_SIZE), query_gain
        ),
        cosine_table,
        sine_table,
    ).astype(jnp.bfloat16)
    rotated_key = (
        apply_rotary(
            final_norm(
                key_matrix.astype(jnp.float32).reshape(tok_count, 1, HEAD_SIZE), key_norm_gain
            ),
            cosine_table,
            sine_table,
        )
        .reshape(tok_count, HEAD_SIZE)
        .astype(jnp.bfloat16)
    )
    packed = jnp.concatenate([rotated_key, values], axis=1)
    query_rows = rotated_query.transpose(1, 0, 2).reshape(head_count * tok_count, HEAD_SIZE)
    score_scale = HEAD_SIZE ** (-0.5)
    start_state = (
        jnp.full((head_count * tok_count,), -1e30, jnp.float32),
        jnp.zeros((head_count * tok_count,), jnp.float32),
        jnp.zeros((head_count * tok_count, HEAD_SIZE), jnp.float32),
    )
    state = start_state
    topk_count = routes.shape[1]
    capacity = max(2, 2 * tok_count * topk_count // (sp_count * tp_count))
    lanes = 2 * HEAD_SIZE
    entries = tok_count * topk_count
    relayed = (
        tp_count == 4
        and sp_count == 2 * tp_count
        and capacity % 16 == 0
        and tok_count % (16 * tp_count) == 0
        and entries % lanes == 0
    )
    if relayed:
        shared_shards = [spread_shards(w, tp_count) for w in (shared_gate, shared_up, shared_down)]
        scale_hi = lax.reduce_precision(route_weights, 8, 7)
        tables = jnp.stack([routes.astype(jnp.float32), scale_hi, route_weights - scale_hi])
        tables = tables.astype(jnp.bfloat16).reshape(-1, lanes)
        table_rows = tables.shape[0]
        tables = jnp.pad(tables, ((0, -table_rows % 16), (0, 0)))
        everything = exchange(jnp.concatenate([packed, tables], axis=0), "sp", 0, True)
        piece = everything[:, :tok_count].reshape(sequence_total, lanes)
        tables = everything[:, tok_count : tok_count + table_rows]
    else:
        piece = exchange(packed, "sp", 0, True).reshape(sequence_total, lanes)
    piece_rows = piece.shape[0]
    block_length = key_block_rows(piece_rows)
    key_blocks = piece.reshape(piece_rows // block_length, block_length, 2 * HEAD_SIZE)

    def step(carry, key_slab):
        run_max, run_total, run_acc = carry
        scores = (
            lax.dot_general(
                query_rows,
                key_slab[:, :HEAD_SIZE],
                (((1,), (1,)), ((), ())),
                preferred_element_type=jnp.float32,
            )
            * score_scale
        )
        new_max = jnp.maximum(run_max, jnp.max(scores, axis=1))
        factor = jnp.exp(run_max - new_max)
        expo_terms = jnp.exp(scores - new_max[:, None])
        new_total = run_total * factor + jnp.sum(expo_terms, axis=1)
        new_acc = run_acc * factor[:, None] + jnp.dot(
            expo_terms.astype(jnp.bfloat16),
            key_slab[:, HEAD_SIZE:],
            preferred_element_type=jnp.float32,
        )
        return ((new_max, new_total, new_acc), None)

    state, _ = lax.scan(step, state, key_blocks)
    run_max, run_total, run_acc = state
    attended = (
        (run_acc / run_total[:, None]).reshape(head_count, tok_count, HEAD_SIZE).transpose(1, 0, 2)
    )
    head_out = final_norm(attended, head_gain.reshape(head_count, HEAD_SIZE)).astype(jnp.bfloat16)
    head_out = head_out.reshape(tok_count, head_count * HEAD_SIZE)
    part_rows = tok_count // tp_count
    token_heads = exchange(
        head_out.reshape(tp_count, part_rows, head_count * HEAD_SIZE), "tp", 1, False
    )
    token_heads = token_heads.transpose(1, 0, 2).reshape(part_rows, -1)
    own_resid = lax.dynamic_slice_in_dim(residual, tp_index * part_rows, part_rows, 0)
    hidden_own = (
        own_resid.astype(jnp.float32)
        + jnp.dot(token_heads, out_proj, preferred_element_type=jnp.float32)
    ).astype(jnp.bfloat16)
    normed_own = final_norm(hidden_own.astype(jnp.float32), ffn_gain).astype(jnp.bfloat16)
    model_width = normed_own.shape[1]
    gate_local = expert_gate[0]
    up_local = expert_up[0]
    down_local = expert_down[0]
    if relayed:
        width = sp_count // tp_count
        sp_index = lax.axis_index("sp")
        stood_for = proxy_plane(tp_index) * width + sp_index % width
        block_tables = lax.dynamic_index_in_dim(tables, stood_for, 0, keepdims=False)
        block_tables = block_tables.astype(jnp.float32).reshape(3, tok_count, topk_count)
        group = width * tp_count
        plane_experts = (sp_index // width) * group + jnp.arange(group, dtype=jnp.int32)
        named = block_tables[0].astype(jnp.int32)[:, :, None] == plane_experts[None, None, :]
        rank = slot_ranks(jnp.any(named, axis=1))
        slots = jnp.arange(capacity, dtype=jnp.int32)
        select = (rank.T[:, None, :] == slots[None, :, None]).astype(jnp.bfloat16)
        chosen = rank[:, :, None] == slots[None, None, :]

        def combine(part):
            scale = jnp.sum(jnp.where(named, block_tables[part][:, :, None], 0.0), axis=1)
            table = jnp.where(chosen, scale[:, :, None], 0.0).astype(jnp.bfloat16)
            return table.reshape(tp_count, part_rows, group * capacity)

        combine_hi, combine_lo = combine(1), combine(2)
        arrived = dispatch(normed_own, select, tp_count, width, tp_count, 2)
        produced = expert_block(
            arrived.reshape(sp_count * capacity, model_width), gate_local, up_local, down_local
        )
        gates, ups, downs = shared_shards
        gate_part = jnp.dot(
            normed_own, jnp.concatenate(gates, axis=1), preferred_element_type=jnp.float32
        )
        up_part = jnp.dot(
            normed_own, jnp.concatenate(ups, axis=1), preferred_element_type=jnp.float32
        )
        shared_inner = (jax.nn.silu(gate_part) * up_part).astype(jnp.bfloat16)
        shared_out = jnp.dot(
            shared_inner, jnp.concatenate(downs, axis=0), preferred_element_type=jnp.float32
        )
        routed = give_back(
            produced.reshape(sp_count, capacity, model_width),
            combine_hi,
            combine_lo,
            tp_count,
            width,
            tp_count,
            3,
        )
        return (
            hidden_own.astype(jnp.float32) + (shared_out + routed.astype(jnp.float32))
        ).astype(jnp.bfloat16)
    normed = exchange(normed_own, "tp", 2, True).reshape(tok_count, model_width)
    slot_total = sp_count * capacity
    experts_here = jnp.arange(sp_count, dtype=jnp.int32) * tp_count + tp_index
    named = routes[:, :, None] == experts_here[None, None, :]
    member = jnp.any(named, axis=1)
    scale = jnp.sum(jnp.where(named, route_weights[:, :, None], 0.0), axis=1)
    rank = slot_ranks(member)
    slots = jnp.arange(capacity, dtype=jnp.int32)
    chosen = rank.T[:, None, :] == slots[None, :, None]
    select = chosen.astype(jnp.bfloat16).reshape(slot_total, tok_count)
    outgoing = jnp.dot(select, normed, preferred_element_type=jnp.float32).astype(jnp.bfloat16)
    arrived = exchange(outgoing.reshape(sp_count, capacity, model_width), "sp", 3, False)
    produced = expert_block(
        arrived.reshape(slot_total, model_width), gate_local, up_local, down_local
    )
    returned = exchange(produced.reshape(sp_count, capacity, model_width), "sp", 4, False).reshape(
        slot_total, model_width
    )
    combine = jnp.where(chosen, scale.T[:, None, :], 0.0).reshape(slot_total, tok_count)
    combine_hi = lax.reduce_precision(combine, 8, 7)
    combine_lo = (combine - combine_hi).astype(jnp.bfloat16)
    combine_hi = combine_hi.astype(jnp.bfloat16)

    def mix(weights):
        return lax.dot_general(
            weights, returned, (((0,), (0,)), ((), ())), preferred_element_type=jnp.float32
        )

    gate_part = jnp.dot(normed, shared_gate, preferred_element_type=jnp.float32)
    up_part = jnp.dot(normed, shared_up, preferred_element_type=jnp.float32)
    shared_inner = (jax.nn.silu(gate_part) * up_part).astype(jnp.bfloat16)
    shares = (
        jnp.dot(shared_inner, shared_down, preferred_element_type=jnp.float32)
        + mix(combine_hi)
        + mix(combine_lo)
    ).astype(jnp.bfloat16)
    shares = exchange(shares.reshape(tp_count, part_rows, model_width), "tp", 5, False)
    mixed_rows = jnp.sum(shares.astype(jnp.float32), axis=0)
    return (hidden_own.astype(jnp.float32) + mixed_rows).astype(jnp.bfloat16)


def solution(mesh):
    placed = (
        P("sp", "tp"),
        P("sp", "tp"),
        P("sp", "tp"),
        P(),
        P(),
        P("tp"),
        P(),
        P("sp", None),
        P(),
        P("sp", None),
        P("sp", None),
        P(("sp", "tp"), None, None),
        P(("sp", "tp"), None, None),
        P(("sp", "tp"), None, None),
        P(None, "tp"),
        P(None, "tp"),
        P("tp", None),
    )
    return jax.shard_map(
        local, mesh=mesh, in_specs=placed, out_specs=P(("sp", "tp"), None), check_vma=False
    )
```

```python
import jax
import jax.numpy as jnp
from jax import lax
from jax.experimental import pallas as pl
from jax.experimental.pallas import tpu as pltpu
from jax.sharding import PartitionSpec as P

HEAD_SIZE = 64
GRID_W = 64


EPS = 1e-06
THETA = 10000.0


def final_norm(field, gain):
    mean_sq = jnp.mean(field * field, axis=-1, keepdims=True)
    return field * lax.rsqrt(mean_sq + EPS) * gain


def grid_tables(positions, sequence_total):
    grid_rows = sequence_total // GRID_W
    row_pos = (positions // GRID_W - grid_rows // 2).astype(jnp.float32)
    col_pos = (positions % GRID_W - GRID_W // 2).astype(jnp.float32)
    quarter = HEAD_SIZE // 4
    inverse = THETA ** (-jnp.arange(quarter, dtype=jnp.float32) / quarter)
    angles = jnp.concatenate([row_pos[:, None] * inverse, col_pos[:, None] * inverse], axis=1)
    return (jnp.cos(angles), jnp.sin(angles))


def apply_rotary(field, cosine_table, sine_table):
    row_count, head_count = (field.shape[0], field.shape[1])
    quarter = HEAD_SIZE // 4
    pieces = field.reshape(row_count, head_count, 2, 2, quarter)
    front_half = pieces[:, :, :, 0, :].reshape(row_count, head_count, 2 * quarter)
    back_half = pieces[:, :, :, 1, :].reshape(row_count, head_count, 2 * quarter)
    cos_wide = cosine_table[:, None, :]
    sin_wide = sine_table[:, None, :]
    new_front = (front_half * cos_wide - back_half * sin_wide).reshape(
        row_count, head_count, 2, 1, quarter
    )
    new_back = (front_half * sin_wide + back_half * cos_wide).reshape(
        row_count, head_count, 2, 1, quarter
    )
    return jnp.concatenate([new_front, new_back], axis=3).reshape(row_count, head_count, HEAD_SIZE)


def exchange(block, axis, call_id, gather):
    count = lax.axis_size(axis)
    if count == 1:
        return block[None] if gather else block
    shape = (count,) + block.shape if gather else block.shape

    def kernel(in_ref, out_ref, send_sems, recv_sems, own_sem):
        me = lax.axis_index(axis)
        barrier = pltpu.get_barrier_semaphore()
        for step in range(1, count):
            pl.semaphore_signal(
                barrier,
                inc=1,
                device_id={axis: lax.rem(me + step, count)},
                device_id_type=pl.DeviceIdType.MESH,
            )
        own = pltpu.make_async_copy(in_ref if gather else in_ref.at[me], out_ref.at[me], own_sem)
        own.start()
        pl.semaphore_wait(barrier, count - 1)
        copies = []
        for step in range(1, count):
            peer = lax.rem(me + step, count)
            copy = pltpu.make_async_remote_copy(
                src_ref=in_ref if gather else in_ref.at[peer],
                dst_ref=out_ref.at[me],
                send_sem=send_sems.at[step],
                recv_sem=recv_sems.at[step],
                device_id={axis: peer},
                device_id_type=pl.DeviceIdType.MESH,
            )
            copy.start()
            copies.append(copy)
        own.wait()
        for copy in copies:
            copy.wait()

    return pl.pallas_call(
        kernel,
        out_shape=jax.ShapeDtypeStruct(shape, block.dtype),
        in_specs=[pl.BlockSpec(memory_space=pltpu.VMEM)],
        out_specs=pl.BlockSpec(memory_space=pltpu.VMEM),
        scratch_shapes=[
            pltpu.SemaphoreType.DMA((count,)),
            pltpu.SemaphoreType.DMA((count,)),
            pltpu.SemaphoreType.DMA,
        ],
        compiler_params=pltpu.CompilerParams(collective_id=call_id, has_side_effects=True),
        name="exchange_%d" % call_id,
    )(block)


def key_block_rows(piece_rows):
    return max((width for width in range(1, 2049) if piece_rows % width == 0))


MESH = pl.DeviceIdType.MESH
COLUMNS = 512


def proxy_plane(t):
    pair, side = t // 2, t % 2
    return pair + side * (3 - 2 * pair)


def proxy_of(plane):
    return jnp.where(plane == 0, 0, jnp.where(plane == 3, 1, plane + 1))


def place(planes, width, tp_count):
    sp, t = lax.axis_index("sp"), lax.axis_index("tp")
    z, x = sp // width, sp % width
    return z, x, t, x * tp_count + t


def greet(z, x, p, planes, width, tp_count):
    barrier = pltpu.get_barrier_semaphore()
    group = width * tp_count
    for step in range(1, group):
        peer = lax.rem(p + step, group)
        pl.semaphore_signal(
            barrier,
            inc=1,
            device_id={"sp": z * width + peer // tp_count, "tp": peer % tp_count},
            device_id_type=MESH,
        )
    for step in (1, planes - 1):
        pl.semaphore_signal(
            barrier,
            inc=1,
            device_id={"sp": lax.rem(z + step, planes) * width + x},
            device_id_type=MESH,
        )
    pl.semaphore_wait(barrier, group - 1 + 2)


def dispatch(normed_own, select, planes, width, tp_count, call_id):
    rows, model = normed_own.shape
    group, capacity, tokens = select.shape
    quarters = tokens // rows

    def kernel(own_ref, sel_ref, out_ref, blk, packed, a_send, z_send, b_recv, c_send, c_recv, sem):
        z, x, t, p = place(planes, width, tp_count)
        zb = proxy_plane(t)
        home = z == zb
        greet(z, x, p, planes, width, tp_count)
        target = proxy_of(z)

        def to_home():
            return pltpu.make_async_remote_copy(
                src_ref=own_ref,
                dst_ref=blk.at[t],
                send_sem=a_send,
                recv_sem=b_recv.at[t],
                device_id={"tp": target},
                device_id_type=MESH,
            )

        @pl.when(t != target)
        def _():
            to_home().start()

        own_copy = pltpu.make_async_copy(own_ref, blk.at[t], sem)

        @pl.when(home)
        def _():
            own_copy.start()
            own_copy.wait()

        def relay(q, up):
            return pltpu.make_async_remote_copy(
                src_ref=blk.at[q],
                dst_ref=blk.at[q],
                send_sem=z_send.at[up, q],
                recv_sem=b_recv.at[q],
                device_id={"sp": (z + (1 if up else -1)) * width + x},
                device_id_type=MESH,
            )

        go_up = (z >= zb) & (z < planes - 1)
        go_down = (z <= zb) & (z > 0)

        for k in range(quarters):
            q = lax.rem(t + k, quarters)

            @pl.when(jnp.logical_not(home & (q == t)))
            def _():
                relay(q, 1).wait_recv()

            @pl.when(go_up)
            def _():
                relay(q, 1).start()

            @pl.when(go_down)
            def _():
                relay(q, 0).start()

        def send(pp):
            return pltpu.make_async_remote_copy(
                src_ref=packed.at[pp],
                dst_ref=out_ref.at[zb * width + x],
                send_sem=c_send.at[pp],
                recv_sem=c_recv.at[zb * width + x],
                device_id={"sp": z * width + pp // tp_count, "tp": pp % tp_count},
                device_id_type=MESH,
            )

        def serve(k, carry):
            pp = lax.rem(p + 1 + k, group)
            chosen = sel_ref[pp]
            for column in range(0, model, COLUMNS):
                part = pl.ds(column, COLUMNS)
                packed[pp, :, part] = jnp.dot(
                    chosen,
                    blk[:, :, part].reshape(tokens, COLUMNS),
                    preferred_element_type=jnp.float32,
                ).astype(jnp.bfloat16)

            @pl.when(pp != p)
            def _():
                send(pp).start()

            return carry

        lax.fori_loop(0, group, serve, 0)
        kept = pltpu.make_async_copy(packed.at[p], out_ref.at[zb * width + x], sem)
        kept.start()
        kept.wait()

        def finish(k, carry):
            pp = lax.rem(p + 1 + k, group)
            send(pp).wait_send()
            source = proxy_plane(pp % tp_count) * width + pp // tp_count
            pltpu.make_async_remote_copy(
                src_ref=packed.at[pp],
                dst_ref=out_ref.at[source],
                send_sem=c_send.at[pp],
                recv_sem=c_recv.at[source],
                device_id={"sp": z * width + pp // tp_count, "tp": pp % tp_count},
                device_id_type=MESH,
            ).wait_recv()
            return carry

        lax.fori_loop(0, group - 1, finish, 0)

        @pl.when(t != target)
        def _():
            to_home().wait_send()

        for q in range(quarters):

            @pl.when(go_up)
            def _():
                relay(q, 1).wait_send()

            @pl.when(go_down)
            def _():
                relay(q, 0).wait_send()

    vmem = pl.BlockSpec(memory_space=pltpu.VMEM)
    dma = pltpu.SemaphoreType.DMA
    return pl.pallas_call(
        kernel,
        out_shape=jax.ShapeDtypeStruct((planes * width, capacity, model), jnp.bfloat16),
        in_specs=[vmem] * 2,
        out_specs=vmem,
        scratch_shapes=[
            pltpu.VMEM((quarters, rows, model), jnp.bfloat16),
            pltpu.VMEM((group, capacity, model), jnp.bfloat16),
            dma,
            dma((2, quarters)),
            dma((quarters,)),
            dma((group,)),
            dma((planes * width,)),
            dma,
        ],
        compiler_params=pltpu.CompilerParams(collective_id=call_id, has_side_effects=True),
        name="dispatch",
    )(normed_own, select)


def give_back(produced, weights_hi, weights_lo, planes, width, tp_count, call_id):
    blocks, capacity, model = produced.shape
    group, quarters = width * tp_count, tp_count
    slots, tokens = weights_hi.shape
    rows = tokens // quarters

    def kernel(
        in_ref, hi_ref, lo_ref, out_ref,
        back, high, low, total, passed, arrived, c_send, c_recv, z_send, z_recv, a_recv, sem,
    ):
        z, x, t, p = place(planes, width, tp_count)
        zb = proxy_plane(t)
        home = z == zb
        greet(z, x, p, planes, width, tp_count)
        keep = pltpu.make_async_copy(in_ref.at[zb * width + x], back.at[p], sem)
        keep.start()

        def send(pp):
            return pltpu.make_async_remote_copy(
                src_ref=in_ref.at[proxy_plane(pp % tp_count) * width + pp // tp_count],
                dst_ref=back.at[p],
                send_sem=c_send.at[pp],
                recv_sem=c_recv.at[p],
                device_id={"sp": z * width + pp // tp_count, "tp": pp % tp_count},
                device_id_type=MESH,
            )

        def came(pp):
            return pltpu.make_async_remote_copy(
                src_ref=in_ref.at[0],
                dst_ref=back.at[pp],
                send_sem=c_send.at[pp],
                recv_sem=c_recv.at[pp],
                device_id={"sp": z * width + pp // tp_count, "tp": pp % tp_count},
                device_id_type=MESH,
            )

        def issue(k, carry):
            rank = k // width
            plane = jnp.where(2 * z < planes, planes - 1 - rank, rank)
            pp = lax.rem(x + k + 1, width) * tp_count + proxy_of(plane)

            @pl.when(pp != p)
            def _():
                send(pp).start()

            return carry

        lax.fori_loop(0, group, issue, 0)
        high[...] = hi_ref[...].T.reshape(quarters, rows, slots)
        low[...] = lo_ref[...].T.reshape(quarters, rows, slots)
        keep.wait()

        def collect(k, carry):
            came(lax.rem(p + 1 + k, group)).wait_recv()
            return carry

        lax.fori_loop(0, group - 1, collect, 0)

        from_above = (z >= zb) & (z < planes - 1)
        from_below = (z <= zb) & (z > 0)

        def hop(q, down):
            return pltpu.make_async_remote_copy(
                src_ref=passed.at[q],
                dst_ref=arrived.at[down, q],
                send_sem=z_send.at[q],
                recv_sem=z_recv.at[down, q],
                device_id={"sp": (z + (-1 if down else 1)) * width + x},
                device_id_type=MESH,
            )

        def to_owner(q):
            return pltpu.make_async_remote_copy(
                src_ref=passed.at[q],
                dst_ref=out_ref,
                send_sem=z_send.at[q],
                recv_sem=a_recv,
                device_id={"tp": q},
                device_id_type=MESH,
            )

        def quarter(q, carry):
            for column in range(0, model, COLUMNS):
                part = pl.ds(column, COLUMNS)
                piece = back[:, :, part].reshape(slots, COLUMNS)
                total[:, part] = jnp.dot(
                    high[q], piece, preferred_element_type=jnp.float32
                ) + jnp.dot(low[q], piece, preferred_element_type=jnp.float32)

            @pl.when(from_above)
            def _():
                hop(q, 1).wait_recv()
                total[...] += arrived[1, q].astype(jnp.float32)

            @pl.when(from_below)
            def _():
                hop(q, 0).wait_recv()
                total[...] += arrived[0, q].astype(jnp.float32)

            passed[q] = total[...].astype(jnp.bfloat16)

            @pl.when(z > zb)
            def _():
                hop(q, 1).start()

            @pl.when(z < zb)
            def _():
                hop(q, 0).start()

            @pl.when(home & (q != t))
            def _():
                to_owner(q).start()

            @pl.when(home & (q == t))
            def _():
                mine = pltpu.make_async_copy(passed.at[q], out_ref, sem)
                mine.start()
                mine.wait()

            return carry

        lax.fori_loop(0, quarters, quarter, 0)

        @pl.when(jnp.logical_not(home))
        def _():
            to_owner(t).wait_recv()

        def sent(k, carry):
            send(lax.rem(p + 1 + k, group)).wait_send()
            return carry

        lax.fori_loop(0, group - 1, sent, 0)

        def left(q, carry):
            @pl.when(jnp.logical_not(home & (q == t)))
            def _():
                to_owner(q).wait_send()

            return carry

        lax.fori_loop(0, quarters, left, 0)

    vmem = pl.BlockSpec(memory_space=pltpu.VMEM)
    dma = pltpu.SemaphoreType.DMA
    return pl.pallas_call(
        kernel,
        out_shape=jax.ShapeDtypeStruct((rows, model), jnp.bfloat16),
        in_specs=[vmem] * 3,
        out_specs=vmem,
        scratch_shapes=[
            pltpu.VMEM((group, capacity, model), jnp.bfloat16),
            pltpu.VMEM((quarters, rows, slots), jnp.bfloat16),
            pltpu.VMEM((quarters, rows, slots), jnp.bfloat16),
            pltpu.VMEM((rows, model), jnp.float32),
            pltpu.VMEM((quarters, rows, model), jnp.bfloat16),
            pltpu.VMEM((2, quarters, rows, model), jnp.bfloat16),
            dma((group,)),
            dma((group,)),
            dma((quarters,)),
            dma((2, quarters)),
            dma,
            dma,
        ],
        compiler_params=pltpu.CompilerParams(collective_id=call_id, has_side_effects=True),
        name="give_back",
    )(produced, weights_hi, weights_lo)


def attend(queries_t, own, gain, tokens, width, call_id):
    count = lax.axis_size("sp")
    planes = count // width
    span = queries_t.shape[1]
    heads = gain.shape[0]
    chunk = 256

    def kernel(q_ref, own_ref, gain_ref, all_ref, out_ref, top, norm, acc, z_send, x_send, recv, sem):
        me = lax.axis_index("sp")
        z, x = me // width, me % width
        beside = z * width + (1 - x)
        barrier = pltpu.get_barrier_semaphore()
        peers = [lax.rem(z + step, planes) * width + x for step in range(1, planes)] + [beside]
        for peer in peers:
            pl.semaphore_signal(barrier, inc=1, device_id={"sp": peer}, device_id_type=MESH)
        kept = pltpu.make_async_copy(own_ref, all_ref.at[me], sem)
        kept.start()
        pl.semaphore_wait(barrier, len(peers))

        def along(step):
            return pltpu.make_async_remote_copy(
                src_ref=own_ref,
                dst_ref=all_ref.at[me],
                send_sem=z_send.at[step],
                recv_sem=recv.at[me],
                device_id={"sp": lax.rem(z + step, planes) * width + x},
                device_id_type=MESH,
            )

        def across(step, column):
            source = lax.rem(z + step, planes) * width + column
            return pltpu.make_async_remote_copy(
                src_ref=own_ref if step == 0 else all_ref.at[source],
                dst_ref=all_ref.at[source],
                send_sem=x_send.at[step],
                recv_sem=recv.at[source],
                device_id={"sp": beside},
                device_id_type=MESH,
            )

        across(0, x).start()
        for step in range(1, planes):
            along(step).start()
        kept.wait()

        def absorb(slot, first):
            keys = all_ref[slot, 0:tokens, 0:HEAD_SIZE]
            vals = all_ref[slot, 0:tokens, HEAD_SIZE : 2 * HEAD_SIZE]
            for start in range(0, span, chunk):
                part = pl.ds(start, chunk)
                scores = jnp.dot(keys, q_ref[:, part], preferred_element_type=jnp.float32)
                peak = jnp.max(scores, axis=0, keepdims=True)
                if not first:
                    old = top[:, part]
                    peak = jnp.maximum(old, peak)
                    factor = jnp.exp(old - peak)
                terms = jnp.exp(scores - peak)
                amount = jnp.sum(terms, axis=0, keepdims=True)
                mixed = lax.dot_general(
                    vals,
                    terms.astype(jnp.bfloat16),
                    (((0,), (0,)), ((), ())),
                    preferred_element_type=jnp.float32,
                )
                if not first:
                    amount = norm[:, part] * factor + amount
                    mixed = acc[:, part] * factor + mixed
                top[:, part] = peak
                norm[:, part] = amount
                acc[:, part] = mixed

        def block(step, column):
            return lax.rem(z + step, planes) * width + column

        absorb(me, True)
        for step in range(1, planes + 1):
            if step < planes:
                across(step, x).wait_recv()
                across(step, x).start()
            across(step - 1, 1 - x).wait_recv()
            absorb(block(step - 1, 1 - x), False)
            if step < planes:
                absorb(block(step, x), False)

        attended = acc[...] / norm[...]
        mean_sq = jnp.mean(attended * attended, axis=0, keepdims=True)
        rows = (attended * lax.rsqrt(mean_sq + EPS)).T
        for h in range(heads):
            out_ref[:, h * HEAD_SIZE : (h + 1) * HEAD_SIZE] = (
                rows[h * tokens : (h + 1) * tokens] * gain_ref[h : h + 1, :]
            ).astype(jnp.bfloat16)
        for step in range(planes):
            if step > 0:
                along(step).wait_send()
            across(step, x).wait_send()

    vmem = pl.BlockSpec(memory_space=pltpu.VMEM)
    dma = pltpu.SemaphoreType.DMA
    return pl.pallas_call(
        kernel,
        out_shape=(
            jax.ShapeDtypeStruct((count,) + own.shape, jnp.bfloat16),
            jax.ShapeDtypeStruct((tokens, heads * HEAD_SIZE), jnp.bfloat16),
        ),
        in_specs=[vmem] * 3,
        out_specs=(vmem, vmem),
        scratch_shapes=[
            pltpu.VMEM((1, span), jnp.float32),
            pltpu.VMEM((1, span), jnp.float32),
            pltpu.VMEM((HEAD_SIZE, span), jnp.float32),
            dma((planes,)),
            dma((planes,)),
            dma((count,)),
            dma,
        ],
        compiler_params=pltpu.CompilerParams(collective_id=call_id, has_side_effects=True),
        name="attend",
    )(queries_t, own, gain)


def scan_attention(query_rows, key_blocks, score_scale):
    start_state = (
        jnp.full((query_rows.shape[0],), -1e30, jnp.float32),
        jnp.zeros((query_rows.shape[0],), jnp.float32),
        jnp.zeros(query_rows.shape, jnp.float32),
    )

    def step(carry, key_slab):
        run_max, run_total, run_acc = carry
        scores = (
            lax.dot_general(
                query_rows,
                key_slab[:, :HEAD_SIZE],
                (((1,), (1,)), ((), ())),
                preferred_element_type=jnp.float32,
            )
            * score_scale
        )
        new_max = jnp.maximum(run_max, jnp.max(scores, axis=1))
        factor = jnp.exp(run_max - new_max)
        expo_terms = jnp.exp(scores - new_max[:, None])
        new_total = run_total * factor + jnp.sum(expo_terms, axis=1)
        new_acc = run_acc * factor[:, None] + jnp.dot(
            expo_terms.astype(jnp.bfloat16),
            key_slab[:, HEAD_SIZE:],
            preferred_element_type=jnp.float32,
        )
        return ((new_max, new_total, new_acc), None)

    (_, run_total, run_acc), _ = lax.scan(step, start_state, key_blocks)
    return run_acc / run_total[:, None]


def spread_shards(shard, tp_count):
    across = lax.ppermute(shard, "tp", [(i, i ^ 2) for i in range(tp_count)])
    beside = [(i, i ^ 1) for i in range(tp_count)]
    return [shard, across, lax.ppermute(shard, "tp", beside), lax.ppermute(across, "tp", beside)]


def slot_ranks(member):
    order = jnp.arange(member.shape[0], dtype=jnp.int32)
    before = (order[:, None] > order[None, :]).astype(jnp.bfloat16)
    rank = jnp.dot(before, member.astype(jnp.bfloat16), preferred_element_type=jnp.float32)
    return jnp.where(member, rank.astype(jnp.int32), -1)


def expert_block(flat_rows, gate_local, up_local, down_local):
    gate_out = jnp.dot(flat_rows, gate_local, preferred_element_type=jnp.float32)
    up_out = jnp.dot(flat_rows, up_local, preferred_element_type=jnp.float32)
    expert_inner = (jax.nn.silu(gate_out) * up_out).astype(jnp.bfloat16)
    return jnp.dot(expert_inner, down_local, preferred_element_type=jnp.float32).astype(
        jnp.bfloat16
    )


def local(
    queries,
    key_matrix,
    values,
    query_gain,
    key_norm_gain,
    head_gain,
    out_proj,
    residual,
    ffn_gain,
    routes,
    route_weights,
    expert_gate,
    expert_up,
    expert_down,
    shared_gate,
    shared_up,
    shared_down,
):
    tok_count = queries.shape[0]
    head_count = queries.shape[1] // HEAD_SIZE
    sp_count = lax.axis_size("sp")
    tp_count = lax.axis_size("tp")
    tp_index = lax.axis_index("tp")
    sequence_total = tok_count * sp_count
    positions = lax.axis_index("sp") * tok_count + jnp.arange(tok_count, dtype=jnp.int32)
    cosine_table, sine_table = grid_tables(positions, sequence_total)
    rotated_query = apply_rotary(
        final_norm(
            queries.astype(jnp.float32).reshape(tok_count, head_count, HEAD_SIZE), query_gain
        ),
        cosine_table,
        sine_table,
    ).astype(jnp.bfloat16)
    rotated_key = (
        apply_rotary(
            final_norm(
                key_matrix.astype(jnp.float32).reshape(tok_count, 1, HEAD_SIZE), key_norm_gain
            ),
            cosine_table,
            sine_table,
        )
        .reshape(tok_count, HEAD_SIZE)
        .astype(jnp.bfloat16)
    )
    packed = jnp.concatenate([rotated_key, values], axis=1)
    score_scale = HEAD_SIZE ** (-0.5)
    topk_count = routes.shape[1]
    capacity = max(2, 2 * tok_count * topk_count // (sp_count * tp_count))
    lanes = 2 * HEAD_SIZE
    entries = tok_count * topk_count
    relayed = (
        tp_count == 4
        and sp_count == 2 * tp_count
        and capacity % 16 == 0
        and tok_count % (16 * tp_count) == 0
        and entries % lanes == 0
        and head_count * tok_count % 256 == 0
    )
    if relayed:
        shared_shards = [spread_shards(w, tp_count) for w in (shared_gate, shared_up, shared_down)]
        scale_hi = lax.reduce_precision(route_weights, 8, 7)
        tables = jnp.stack([routes.astype(jnp.float32), scale_hi, route_weights - scale_hi])
        tables = tables.astype(jnp.bfloat16).reshape(-1, lanes)
        table_rows = tables.shape[0]
        tables = jnp.pad(tables, ((0, -table_rows % 16), (0, 0)))
        scaled = rotated_query * jnp.asarray(score_scale, jnp.bfloat16)
        everything, head_out = attend(
            scaled.transpose(2, 1, 0).reshape(HEAD_SIZE, head_count * tok_count),
            jnp.concatenate([packed, tables], axis=0),
            head_gain.reshape(head_count, HEAD_SIZE),
            tok_count,
            sp_count // tp_count,
            0,
        )
        tables = everything[:, tok_count : tok_count + table_rows]
    else:
        piece = exchange(packed, "sp", 0, True).reshape(sequence_total, lanes)
        query_rows = rotated_query.transpose(1, 0, 2).reshape(head_count * tok_count, HEAD_SIZE)
        block_length = key_block_rows(sequence_total)
        key_blocks = piece.reshape(sequence_total // block_length, block_length, lanes)
        attended = scan_attention(query_rows, key_blocks, score_scale)
        attended = attended.reshape(head_count, tok_count, HEAD_SIZE).transpose(1, 0, 2)
        head_out = final_norm(attended, head_gain.reshape(head_count, HEAD_SIZE))
        head_out = head_out.astype(jnp.bfloat16).reshape(tok_count, head_count * HEAD_SIZE)
    part_rows = tok_count // tp_count
    token_heads = exchange(
        head_out.reshape(tp_count, part_rows, head_count * HEAD_SIZE), "tp", 1, False
    )
    token_heads = token_heads.transpose(1, 0, 2).reshape(part_rows, -1)
    own_resid = lax.dynamic_slice_in_dim(residual, tp_index * part_rows, part_rows, 0)
    hidden_own = (
        own_resid.astype(jnp.float32)
        + jnp.dot(token_heads, out_proj, preferred_element_type=jnp.float32)
    ).astype(jnp.bfloat16)
    normed_own = final_norm(hidden_own.astype(jnp.float32), ffn_gain).astype(jnp.bfloat16)
    model_width = normed_own.shape[1]
    gate_local = expert_gate[0]
    up_local = expert_up[0]
    down_local = expert_down[0]
    if relayed:
        width = sp_count // tp_count
        sp_index = lax.axis_index("sp")
        stood_for = proxy_plane(tp_index) * width + sp_index % width
        block_tables = lax.dynamic_index_in_dim(tables, stood_for, 0, keepdims=False)
        block_tables = block_tables.astype(jnp.float32).reshape(3, tok_count, topk_count)
        group = width * tp_count
        plane_experts = (sp_index // width) * group + jnp.arange(group, dtype=jnp.int32)
        named = block_tables[0].astype(jnp.int32)[:, :, None] == plane_experts[None, None, :]
        rank = slot_ranks(jnp.any(named, axis=1))
        slots = jnp.arange(capacity, dtype=jnp.int32)
        select = (rank.T[:, None, :] == slots[None, :, None]).astype(jnp.bfloat16)

        def combine(part):
            scale = jnp.sum(jnp.where(named, block_tables[part][:, :, None], 0.0), axis=1)
            table = select * scale.T.astype(jnp.bfloat16)[:, None, :]
            return table.reshape(group * capacity, tok_count)

        combine_hi, combine_lo = combine(1), combine(2)
        arrived = dispatch(normed_own, select, tp_count, width, tp_count, 2)
        produced = expert_block(
            arrived.reshape(sp_count * capacity, model_width), gate_local, up_local, down_local
        )
        gates, ups, downs = shared_shards
        gate_part = jnp.dot(
            normed_own, jnp.concatenate(gates, axis=1), preferred_element_type=jnp.float32
        )
        up_part = jnp.dot(
            normed_own, jnp.concatenate(ups, axis=1), preferred_element_type=jnp.float32
        )
        shared_inner = (jax.nn.silu(gate_part) * up_part).astype(jnp.bfloat16)
        shared_out = jnp.dot(
            shared_inner, jnp.concatenate(downs, axis=0), preferred_element_type=jnp.float32
        )
        routed = give_back(
            produced.reshape(sp_count, capacity, model_width),
            combine_hi,
            combine_lo,
            tp_count,
            width,
            tp_count,
            3,
        )
        return (
            hidden_own.astype(jnp.float32) + (shared_out + routed.astype(jnp.float32))
        ).astype(jnp.bfloat16)
    normed = exchange(normed_own, "tp", 2, True).reshape(tok_count, model_width)
    slot_total = sp_count * capacity
    experts_here = jnp.arange(sp_count, dtype=jnp.int32) * tp_count + tp_index
    named = routes[:, :, None] == experts_here[None, None, :]
    member = jnp.any(named, axis=1)
    scale = jnp.sum(jnp.where(named, route_weights[:, :, None], 0.0), axis=1)
    rank = slot_ranks(member)
    slots = jnp.arange(capacity, dtype=jnp.int32)
    chosen = rank.T[:, None, :] == slots[None, :, None]
    select = chosen.astype(jnp.bfloat16).reshape(slot_total, tok_count)
    outgoing = jnp.dot(select, normed, preferred_element_type=jnp.float32).astype(jnp.bfloat16)
    arrived = exchange(outgoing.reshape(sp_count, capacity, model_width), "sp", 3, False)
    produced = expert_block(
        arrived.reshape(slot_total, model_width), gate_local, up_local, down_local
    )
    returned = exchange(produced.reshape(sp_count, capacity, model_width), "sp", 4, False).reshape(
        slot_total, model_width
    )
    combine = jnp.where(chosen, scale.T[:, None, :], 0.0).reshape(slot_total, tok_count)
    combine_hi = lax.reduce_precision(combine, 8, 7)
    combine_lo = (combine - combine_hi).astype(jnp.bfloat16)
    combine_hi = combine_hi.astype(jnp.bfloat16)

    def mix(weights):
        return lax.dot_general(
            weights, returned, (((0,), (0,)), ((), ())), preferred_element_type=jnp.float32
        )

    gate_part = jnp.dot(normed, shared_gate, preferred_element_type=jnp.float32)
    up_part = jnp.dot(normed, shared_up, preferred_element_type=jnp.float32)
    shared_inner = (jax.nn.silu(gate_part) * up_part).astype(jnp.bfloat16)
    shares = (
        jnp.dot(shared_inner, shared_down, preferred_element_type=jnp.float32)
        + mix(combine_hi)
        + mix(combine_lo)
    ).astype(jnp.bfloat16)
    shares = exchange(shares.reshape(tp_count, part_rows, model_width), "tp", 5, False)
    mixed_rows = jnp.sum(shares.astype(jnp.float32), axis=0)
    return (hidden_own.astype(jnp.float32) + mixed_rows).astype(jnp.bfloat16)


def solution(mesh):
    placed = (
        P("sp", "tp"),
        P("sp", "tp"),
        P("sp", "tp"),
        P(),
        P(),
        P("tp"),
        P(),
        P("sp", None),
        P(),
        P("sp", None),
        P("sp", None),
        P(("sp", "tp"), None, None),
        P(("sp", "tp"), None, None),
        P(("sp", "tp"), None, None),
        P(None, "tp"),
        P(None, "tp"),
        P("tp", None),
    )
    return jax.shard_map(
        local, mesh=mesh, in_specs=placed, out_specs=P(("sp", "tp"), None), check_vma=False
    )
```

```python
import jax
import jax.numpy as jnp
from jax import lax
from jax.experimental import pallas as pl
from jax.experimental.pallas import tpu as pltpu
from jax.sharding import PartitionSpec as P

HEAD_SIZE = 64
GRID_W = 64


EPS = 1e-06
THETA = 10000.0


def final_norm(field, gain):
    mean_sq = jnp.mean(field * field, axis=-1, keepdims=True)
    return field * lax.rsqrt(mean_sq + EPS) * gain


def grid_tables(positions, sequence_total):
    grid_rows = sequence_total // GRID_W
    row_pos = (positions // GRID_W - grid_rows // 2).astype(jnp.float32)
    col_pos = (positions % GRID_W - GRID_W // 2).astype(jnp.float32)
    quarter = HEAD_SIZE // 4
    inverse = THETA ** (-jnp.arange(quarter, dtype=jnp.float32) / quarter)
    angles = jnp.concatenate([row_pos[:, None] * inverse, col_pos[:, None] * inverse], axis=1)
    return (jnp.cos(angles), jnp.sin(angles))


def apply_rotary(field, cosine_table, sine_table):
    row_count, head_count = (field.shape[0], field.shape[1])
    quarter = HEAD_SIZE // 4
    pieces = field.reshape(row_count, head_count, 2, 2, quarter)
    front_half = pieces[:, :, :, 0, :].reshape(row_count, head_count, 2 * quarter)
    back_half = pieces[:, :, :, 1, :].reshape(row_count, head_count, 2 * quarter)
    cos_wide = cosine_table[:, None, :]
    sin_wide = sine_table[:, None, :]
    new_front = (front_half * cos_wide - back_half * sin_wide).reshape(
        row_count, head_count, 2, 1, quarter
    )
    new_back = (front_half * sin_wide + back_half * cos_wide).reshape(
        row_count, head_count, 2, 1, quarter
    )
    return jnp.concatenate([new_front, new_back], axis=3).reshape(row_count, head_count, HEAD_SIZE)


def exchange(block, axis, call_id, gather):
    count = lax.axis_size(axis)
    if count == 1:
        return block[None] if gather else block
    shape = (count,) + block.shape if gather else block.shape

    def kernel(in_ref, out_ref, send_sems, recv_sems, own_sem):
        me = lax.axis_index(axis)
        barrier = pltpu.get_barrier_semaphore()
        for step in range(1, count):
            pl.semaphore_signal(
                barrier,
                inc=1,
                device_id={axis: lax.rem(me + step, count)},
                device_id_type=pl.DeviceIdType.MESH,
            )
        own = pltpu.make_async_copy(in_ref if gather else in_ref.at[me], out_ref.at[me], own_sem)
        own.start()
        pl.semaphore_wait(barrier, count - 1)
        copies = []
        for step in range(1, count):
            peer = lax.rem(me + step, count)
            copy = pltpu.make_async_remote_copy(
                src_ref=in_ref if gather else in_ref.at[peer],
                dst_ref=out_ref.at[me],
                send_sem=send_sems.at[step],
                recv_sem=recv_sems.at[step],
                device_id={axis: peer},
                device_id_type=pl.DeviceIdType.MESH,
            )
            copy.start()
            copies.append(copy)
        own.wait()
        for copy in copies:
            copy.wait()

    return pl.pallas_call(
        kernel,
        out_shape=jax.ShapeDtypeStruct(shape, block.dtype),
        in_specs=[pl.BlockSpec(memory_space=pltpu.VMEM)],
        out_specs=pl.BlockSpec(memory_space=pltpu.VMEM),
        scratch_shapes=[
            pltpu.SemaphoreType.DMA((count,)),
            pltpu.SemaphoreType.DMA((count,)),
            pltpu.SemaphoreType.DMA,
        ],
        compiler_params=pltpu.CompilerParams(collective_id=call_id, has_side_effects=True),
        name="exchange_%d" % call_id,
    )(block)


def key_block_rows(piece_rows):
    return max((width for width in range(1, 2049) if piece_rows % width == 0))


MESH = pl.DeviceIdType.MESH
COLUMNS = 512


def proxy_plane(t):
    pair, side = t // 2, t % 2
    return pair + side * (3 - 2 * pair)


def proxy_of(plane):
    return jnp.where(plane == 0, 0, jnp.where(plane == 3, 1, plane + 1))


def place(planes, width, tp_count):
    sp, t = lax.axis_index("sp"), lax.axis_index("tp")
    z, x = sp // width, sp % width
    return z, x, t, x * tp_count + t


def greet(z, x, p, planes, width, tp_count):
    barrier = pltpu.get_barrier_semaphore()
    group = width * tp_count
    for step in range(1, group):
        peer = lax.rem(p + step, group)
        pl.semaphore_signal(
            barrier,
            inc=1,
            device_id={"sp": z * width + peer // tp_count, "tp": peer % tp_count},
            device_id_type=MESH,
        )
    for step in (1, planes - 1):
        pl.semaphore_signal(
            barrier,
            inc=1,
            device_id={"sp": lax.rem(z + step, planes) * width + x},
            device_id_type=MESH,
        )
    pl.semaphore_wait(barrier, group - 1 + 2)


def dispatch(normed_own, select, shards, planes, width, tp_count, call_id):
    rows, model = normed_own.shape
    group, capacity, tokens = select.shape
    quarters = tokens // rows

    given = len(shards)

    def kernel(own_ref, sel_ref, *refs):
        shard_refs, out_ref, pair_refs = refs[:given], refs[given], refs[given + 1 : 2 * given + 1]
        blk, packed, a_send, z_send, b_recv, c_send, c_recv, w_send, w_recv, sem = refs[
            2 * given + 1 :
        ]
        z, x, t, p = place(planes, width, tp_count)
        zb = proxy_plane(t)
        home = z == zb
        greet(z, x, p, planes, width, tp_count)
        target = proxy_of(z)

        def to_home():
            return pltpu.make_async_remote_copy(
                src_ref=own_ref,
                dst_ref=blk.at[t],
                send_sem=a_send,
                recv_sem=b_recv.at[t],
                device_id={"tp": target},
                device_id_type=MESH,
            )

        @pl.when(t != target)
        def _():
            to_home().start()

        pairs = [
            pltpu.make_async_remote_copy(
                src_ref=shard_refs[i],
                dst_ref=pair_refs[i],
                send_sem=w_send.at[i],
                recv_sem=w_recv.at[i],
                device_id={"tp": t + 1 - 2 * lax.rem(t, 2)},
                device_id_type=MESH,
            )
            for i in range(given)
        ]
        for copy in pairs:
            copy.start()
        own_copy = pltpu.make_async_copy(own_ref, blk.at[t], sem)

        @pl.when(home)
        def _():
            own_copy.start()
            own_copy.wait()

        def relay(q, up):
            return pltpu.make_async_remote_copy(
                src_ref=blk.at[q],
                dst_ref=blk.at[q],
                send_sem=z_send.at[up, q],
                recv_sem=b_recv.at[q],
                device_id={"sp": (z + (1 if up else -1)) * width + x},
                device_id_type=MESH,
            )

        go_up = (z >= zb) & (z < planes - 1)
        go_down = (z <= zb) & (z > 0)

        for k in range(quarters):
            q = lax.rem(t + k, quarters)

            @pl.when(jnp.logical_not(home & (q == t)))
            def _():
                relay(q, 1).wait_recv()

            @pl.when(go_up)
            def _():
                relay(q, 1).start()

            @pl.when(go_down)
            def _():
                relay(q, 0).start()

        def send(pp):
            return pltpu.make_async_remote_copy(
                src_ref=packed.at[pp],
                dst_ref=out_ref.at[zb * width + x],
                send_sem=c_send.at[pp],
                recv_sem=c_recv.at[zb * width + x],
                device_id={"sp": z * width + pp // tp_count, "tp": pp % tp_count},
                device_id_type=MESH,
            )

        def serve(k, carry):
            pp = lax.rem(p + 1 + k, group)
            chosen = sel_ref[pp]
            for column in range(0, model, COLUMNS):
                part = pl.ds(column, COLUMNS)
                packed[pp, :, part] = jnp.dot(
                    chosen,
                    blk[:, :, part].reshape(tokens, COLUMNS),
                    preferred_element_type=jnp.float32,
                ).astype(jnp.bfloat16)

            @pl.when(pp != p)
            def _():
                send(pp).start()

            return carry

        lax.fori_loop(0, group, serve, 0)
        kept = pltpu.make_async_copy(packed.at[p], out_ref.at[zb * width + x], sem)
        kept.start()
        kept.wait()

        def finish(k, carry):
            pp = lax.rem(p + 1 + k, group)
            send(pp).wait_send()
            source = proxy_plane(pp % tp_count) * width + pp // tp_count
            pltpu.make_async_remote_copy(
                src_ref=packed.at[pp],
                dst_ref=out_ref.at[source],
                send_sem=c_send.at[pp],
                recv_sem=c_recv.at[source],
                device_id={"sp": z * width + pp // tp_count, "tp": pp % tp_count},
                device_id_type=MESH,
            ).wait_recv()
            return carry

        lax.fori_loop(0, group - 1, finish, 0)

        @pl.when(t != target)
        def _():
            to_home().wait_send()

        for q in range(quarters):

            @pl.when(go_up)
            def _():
                relay(q, 1).wait_send()

            @pl.when(go_down)
            def _():
                relay(q, 0).wait_send()

        for copy in pairs:
            copy.wait()

    vmem = pl.BlockSpec(memory_space=pltpu.VMEM)
    dma = pltpu.SemaphoreType.DMA
    return pl.pallas_call(
        kernel,
        out_shape=[jax.ShapeDtypeStruct((planes * width, capacity, model), jnp.bfloat16)]
        + [jax.ShapeDtypeStruct(w.shape, w.dtype) for w in shards],
        in_specs=[vmem] * 2 + [pl.BlockSpec(memory_space=pl.ANY)] * given,
        out_specs=[vmem] + [pl.BlockSpec(memory_space=pl.ANY)] * given,
        scratch_shapes=[
            pltpu.VMEM((quarters, rows, model), jnp.bfloat16),
            pltpu.VMEM((group, capacity, model), jnp.bfloat16),
            dma,
            dma((2, quarters)),
            dma((quarters,)),
            dma((group,)),
            dma((planes * width,)),
            dma((given,)),
            dma((given,)),
            dma,
        ],
        compiler_params=pltpu.CompilerParams(collective_id=call_id, has_side_effects=True),
        name="dispatch",
    )(normed_own, select, *shards)


def give_back(produced, weights_hi, weights_lo, own, shards, planes, width, tp_count, call_id):
    blocks, capacity, model = produced.shape
    group, quarters = width * tp_count, tp_count
    slots, tokens = weights_hi.shape
    rows = tokens // quarters

    pieces = len(shards) // 3

    def kernel(in_ref, hi_ref, lo_ref, own_ref, *refs):
        gates, ups = refs[:pieces], refs[pieces : 2 * pieces]
        downs, refs = refs[2 * pieces : 3 * pieces], refs[3 * pieces :]
        out_ref, shared_ref, back, high, low, total, passed, arrived = refs[:8]
        c_send, c_recv, z_send, z_recv, a_recv, sem = refs[8:]
        z, x, t, p = place(planes, width, tp_count)
        zb = proxy_plane(t)
        home = z == zb
        greet(z, x, p, planes, width, tp_count)
        keep = pltpu.make_async_copy(in_ref.at[zb * width + x], back.at[p], sem)
        keep.start()

        def send(pp):
            return pltpu.make_async_remote_copy(
                src_ref=in_ref.at[proxy_plane(pp % tp_count) * width + pp // tp_count],
                dst_ref=back.at[p],
                send_sem=c_send.at[pp],
                recv_sem=c_recv.at[p],
                device_id={"sp": z * width + pp // tp_count, "tp": pp % tp_count},
                device_id_type=MESH,
            )

        def came(pp):
            return pltpu.make_async_remote_copy(
                src_ref=in_ref.at[0],
                dst_ref=back.at[pp],
                send_sem=c_send.at[pp],
                recv_sem=c_recv.at[pp],
                device_id={"sp": z * width + pp // tp_count, "tp": pp % tp_count},
                device_id_type=MESH,
            )

        def issue(k, carry):
            rank = k // width
            plane = jnp.where(2 * z < planes, planes - 1 - rank, rank)
            pp = lax.rem(x + k + 1, width) * tp_count + proxy_of(plane)

            @pl.when(pp != p)
            def _():
                send(pp).start()

            return carry

        lax.fori_loop(0, group, issue, 0)
        high[...] = hi_ref[...].T.reshape(quarters, rows, slots)
        low[...] = lo_ref[...].T.reshape(quarters, rows, slots)
        for i in range(pieces):
            gate = jnp.dot(own_ref[...], gates[i][...], preferred_element_type=jnp.float32)
            up = jnp.dot(own_ref[...], ups[i][...], preferred_element_type=jnp.float32)
            inner = (gate / (1.0 + jnp.exp(-gate)) * up).astype(jnp.bfloat16)
            for column in range(0, model, COLUMNS):
                part = pl.ds(column, COLUMNS)
                share = jnp.dot(inner, downs[i][:, part], preferred_element_type=jnp.float32)
                if i == 0:
                    shared_ref[:, part] = share
                else:
                    shared_ref[:, part] += share
        keep.wait()

        def collect(k, carry):
            came(lax.rem(p + 1 + k, group)).wait_recv()
            return carry

        lax.fori_loop(0, group - 1, collect, 0)

        from_above = (z >= zb) & (z < planes - 1)
        from_below = (z <= zb) & (z > 0)

        def hop(q, down):
            return pltpu.make_async_remote_copy(
                src_ref=passed.at[q],
                dst_ref=arrived.at[down, q],
                send_sem=z_send.at[q],
                recv_sem=z_recv.at[down, q],
                device_id={"sp": (z + (-1 if down else 1)) * width + x},
                device_id_type=MESH,
            )

        def to_owner(q):
            return pltpu.make_async_remote_copy(
                src_ref=passed.at[q],
                dst_ref=out_ref,
                send_sem=z_send.at[q],
                recv_sem=a_recv,
                device_id={"tp": q},
                device_id_type=MESH,
            )

        def quarter(q, carry):
            for column in range(0, model, COLUMNS):
                part = pl.ds(column, COLUMNS)
                piece = back[:, :, part].reshape(slots, COLUMNS)
                total[:, part] = jnp.dot(
                    high[q], piece, preferred_element_type=jnp.float32
                ) + jnp.dot(low[q], piece, preferred_element_type=jnp.float32)

            @pl.when(from_above)
            def _():
                hop(q, 1).wait_recv()
                total[...] += arrived[1, q].astype(jnp.float32)

            @pl.when(from_below)
            def _():
                hop(q, 0).wait_recv()
                total[...] += arrived[0, q].astype(jnp.float32)

            passed[q] = total[...].astype(jnp.bfloat16)

            @pl.when(z > zb)
            def _():
                hop(q, 1).start()

            @pl.when(z < zb)
            def _():
                hop(q, 0).start()

            @pl.when(home & (q != t))
            def _():
                to_owner(q).start()

            @pl.when(home & (q == t))
            def _():
                mine = pltpu.make_async_copy(passed.at[q], out_ref, sem)
                mine.start()
                mine.wait()

            return carry

        lax.fori_loop(0, quarters, quarter, 0)

        @pl.when(jnp.logical_not(home))
        def _():
            to_owner(t).wait_recv()

        def sent(k, carry):
            send(lax.rem(p + 1 + k, group)).wait_send()
            return carry

        lax.fori_loop(0, group - 1, sent, 0)

        def left(q, carry):
            @pl.when(jnp.logical_not(home & (q == t)))
            def _():
                to_owner(q).wait_send()

            return carry

        lax.fori_loop(0, quarters, left, 0)

    vmem = pl.BlockSpec(memory_space=pltpu.VMEM)
    dma = pltpu.SemaphoreType.DMA
    return pl.pallas_call(
        kernel,
        out_shape=(
            jax.ShapeDtypeStruct((rows, model), jnp.bfloat16),
            jax.ShapeDtypeStruct((rows, model), jnp.float32),
        ),
        in_specs=[vmem] * (4 + 3 * pieces),
        out_specs=(vmem, vmem),
        scratch_shapes=[
            pltpu.VMEM((group, capacity, model), jnp.bfloat16),
            pltpu.VMEM((quarters, rows, slots), jnp.bfloat16),
            pltpu.VMEM((quarters, rows, slots), jnp.bfloat16),
            pltpu.VMEM((rows, model), jnp.float32),
            pltpu.VMEM((quarters, rows, model), jnp.bfloat16),
            pltpu.VMEM((2, quarters, rows, model), jnp.bfloat16),
            dma((group,)),
            dma((group,)),
            dma((quarters,)),
            dma((2, quarters)),
            dma,
            dma,
        ],
        compiler_params=pltpu.CompilerParams(collective_id=call_id, has_side_effects=True),
        name="give_back",
    )(produced, weights_hi, weights_lo, own, *shards)


def attend(queries_t, own, gain, tokens, width, tp_count, call_id):
    count = lax.axis_size("sp")
    planes = count // width
    span = queries_t.shape[1]
    heads = gain.shape[0]
    chunk = 256

    rows_each = tokens // tp_count
    features = heads * HEAD_SIZE

    def kernel(
        q_ref, own_ref, gain_ref, all_ref, heads_ref,
        out_ref, top, norm, acc, z_send, x_send, recv, h_send, h_recv, sem,
    ):
        me, t = lax.axis_index("sp"), lax.axis_index("tp")
        z, x = me // width, me % width
        beside = z * width + (1 - x)
        barrier = pltpu.get_barrier_semaphore()
        peers = [lax.rem(z + step, planes) * width + x for step in range(1, planes)] + [beside]
        for peer in peers:
            pl.semaphore_signal(barrier, inc=1, device_id={"sp": peer}, device_id_type=MESH)
        for step in range(1, tp_count):
            pl.semaphore_signal(
                barrier,
                inc=1,
                device_id={"tp": lax.rem(t + step, tp_count)},
                device_id_type=MESH,
            )
        kept = pltpu.make_async_copy(own_ref, all_ref.at[me], sem)
        kept.start()
        pl.semaphore_wait(barrier, len(peers) + tp_count - 1)

        def along(step):
            return pltpu.make_async_remote_copy(
                src_ref=own_ref,
                dst_ref=all_ref.at[me],
                send_sem=z_send.at[step],
                recv_sem=recv.at[me],
                device_id={"sp": lax.rem(z + step, planes) * width + x},
                device_id_type=MESH,
            )

        def across(step, column):
            source = lax.rem(z + step, planes) * width + column
            return pltpu.make_async_remote_copy(
                src_ref=own_ref if step == 0 else all_ref.at[source],
                dst_ref=all_ref.at[source],
                send_sem=x_send.at[step],
                recv_sem=recv.at[source],
                device_id={"sp": beside},
                device_id_type=MESH,
            )

        across(0, x).start()
        for step in range(1, planes):
            along(step).start()
        kept.wait()

        def absorb(slot, first):
            keys = all_ref[slot, 0:tokens, 0:HEAD_SIZE]
            vals = all_ref[slot, 0:tokens, HEAD_SIZE : 2 * HEAD_SIZE]
            for start in range(0, span, chunk):
                part = pl.ds(start, chunk)
                scores = jnp.dot(keys, q_ref[:, part], preferred_element_type=jnp.float32)
                peak = jnp.max(scores, axis=0, keepdims=True)
                if not first:
                    old = top[:, part]
                    peak = jnp.maximum(old, peak)
                    factor = jnp.exp(old - peak)
                terms = jnp.exp(scores - peak)
                amount = jnp.sum(terms, axis=0, keepdims=True)
                mixed = lax.dot_general(
                    vals,
                    terms.astype(jnp.bfloat16),
                    (((0,), (0,)), ((), ())),
                    preferred_element_type=jnp.float32,
                )
                if not first:
                    amount = norm[:, part] * factor + amount
                    mixed = acc[:, part] * factor + mixed
                top[:, part] = peak
                norm[:, part] = amount
                acc[:, part] = mixed

        def block(step, column):
            return lax.rem(z + step, planes) * width + column

        absorb(me, True)
        for step in range(1, planes + 1):
            if step < planes:
                across(step, x).wait_recv()
                across(step, x).start()
            across(step - 1, 1 - x).wait_recv()
            absorb(block(step - 1, 1 - x), False)
            if step < planes:
                absorb(block(step, x), False)

        attended = acc[...] / norm[...]
        mean_sq = jnp.mean(attended * attended, axis=0, keepdims=True)
        rows = (attended * lax.rsqrt(mean_sq + EPS)).T
        for h in range(heads):
            out_ref[:, h * HEAD_SIZE : (h + 1) * HEAD_SIZE] = (
                rows[h * tokens : (h + 1) * tokens] * gain_ref[h : h + 1, :]
            ).astype(jnp.bfloat16)
        mine = heads_ref.at[:, pl.ds(pl.multiple_of(t * features, 128), features)]

        def part_of(peer):
            return out_ref.at[pl.ds(pl.multiple_of(peer * rows_each, 16), rows_each)]

        swaps = []
        for step in range(1, tp_count):
            peer = lax.rem(t + step, tp_count)
            swap = pltpu.make_async_remote_copy(
                src_ref=part_of(peer),
                dst_ref=mine,
                send_sem=h_send.at[step],
                recv_sem=h_recv.at[step],
                device_id={"tp": peer},
                device_id_type=MESH,
            )
            swap.start()
            swaps.append(swap)
        kept = pltpu.make_async_copy(part_of(t), mine, sem)
        kept.start()
        kept.wait()
        for swap in swaps:
            swap.wait()
        for step in range(planes):
            if step > 0:
                along(step).wait_send()
            across(step, x).wait_send()

    vmem = pl.BlockSpec(memory_space=pltpu.VMEM)
    dma = pltpu.SemaphoreType.DMA
    return pl.pallas_call(
        kernel,
        out_shape=(
            jax.ShapeDtypeStruct((count,) + own.shape, jnp.bfloat16),
            jax.ShapeDtypeStruct((rows_each, tp_count * features), jnp.bfloat16),
        ),
        in_specs=[vmem] * 3,
        out_specs=(vmem, vmem),
        scratch_shapes=[
            pltpu.VMEM((tokens, features), jnp.bfloat16),
            pltpu.VMEM((1, span), jnp.float32),
            pltpu.VMEM((1, span), jnp.float32),
            pltpu.VMEM((HEAD_SIZE, span), jnp.float32),
            dma((planes,)),
            dma((planes,)),
            dma((count,)),
            dma((tp_count,)),
            dma((tp_count,)),
            dma,
        ],
        compiler_params=pltpu.CompilerParams(collective_id=call_id, has_side_effects=True),
        name="attend",
    )(queries_t, own, gain)


def scan_attention(query_rows, key_blocks, score_scale):
    start_state = (
        jnp.full((query_rows.shape[0],), -1e30, jnp.float32),
        jnp.zeros((query_rows.shape[0],), jnp.float32),
        jnp.zeros(query_rows.shape, jnp.float32),
    )

    def step(carry, key_slab):
        run_max, run_total, run_acc = carry
        scores = (
            lax.dot_general(
                query_rows,
                key_slab[:, :HEAD_SIZE],
                (((1,), (1,)), ((), ())),
                preferred_element_type=jnp.float32,
            )
            * score_scale
        )
        new_max = jnp.maximum(run_max, jnp.max(scores, axis=1))
        factor = jnp.exp(run_max - new_max)
        expo_terms = jnp.exp(scores - new_max[:, None])
        new_total = run_total * factor + jnp.sum(expo_terms, axis=1)
        new_acc = run_acc * factor[:, None] + jnp.dot(
            expo_terms.astype(jnp.bfloat16),
            key_slab[:, HEAD_SIZE:],
            preferred_element_type=jnp.float32,
        )
        return ((new_max, new_total, new_acc), None)

    (_, run_total, run_acc), _ = lax.scan(step, start_state, key_blocks)
    return run_acc / run_total[:, None]


def across_pairs(shard, tp_count):
    return lax.ppermute(shard, "tp", [(i, i ^ 2) for i in range(tp_count)])


def slot_ranks(member):
    order = jnp.arange(member.shape[0], dtype=jnp.int32)
    before = (order[:, None] > order[None, :]).astype(jnp.bfloat16)
    rank = jnp.dot(before, member.astype(jnp.bfloat16), preferred_element_type=jnp.float32)
    return jnp.where(member, rank.astype(jnp.int32), -1)


def expert_block(flat_rows, gate_local, up_local, down_local):
    gate_out = jnp.dot(flat_rows, gate_local, preferred_element_type=jnp.float32)
    up_out = jnp.dot(flat_rows, up_local, preferred_element_type=jnp.float32)
    expert_inner = (jax.nn.silu(gate_out) * up_out).astype(jnp.bfloat16)
    return jnp.dot(expert_inner, down_local, preferred_element_type=jnp.float32).astype(
        jnp.bfloat16
    )


def local(
    queries,
    key_matrix,
    values,
    query_gain,
    key_norm_gain,
    head_gain,
    out_proj,
    residual,
    ffn_gain,
    routes,
    route_weights,
    expert_gate,
    expert_up,
    expert_down,
    shared_gate,
    shared_up,
    shared_down,
):
    tok_count = queries.shape[0]
    head_count = queries.shape[1] // HEAD_SIZE
    sp_count = lax.axis_size("sp")
    tp_count = lax.axis_size("tp")
    tp_index = lax.axis_index("tp")
    sequence_total = tok_count * sp_count
    positions = lax.axis_index("sp") * tok_count + jnp.arange(tok_count, dtype=jnp.int32)
    cosine_table, sine_table = grid_tables(positions, sequence_total)
    rotated_query = apply_rotary(
        final_norm(
            queries.astype(jnp.float32).reshape(tok_count, head_count, HEAD_SIZE), query_gain
        ),
        cosine_table,
        sine_table,
    ).astype(jnp.bfloat16)
    rotated_key = (
        apply_rotary(
            final_norm(
                key_matrix.astype(jnp.float32).reshape(tok_count, 1, HEAD_SIZE), key_norm_gain
            ),
            cosine_table,
            sine_table,
        )
        .reshape(tok_count, HEAD_SIZE)
        .astype(jnp.bfloat16)
    )
    packed = jnp.concatenate([rotated_key, values], axis=1)
    score_scale = HEAD_SIZE ** (-0.5)
    topk_count = routes.shape[1]
    capacity = max(2, 2 * tok_count * topk_count // (sp_count * tp_count))
    lanes = 2 * HEAD_SIZE
    entries = tok_count * topk_count
    relayed = (
        tp_count == 4
        and sp_count == 2 * tp_count
        and capacity % 16 == 0
        and tok_count % (16 * tp_count) == 0
        and entries % lanes == 0
        and head_count * tok_count % 256 == 0
        and head_count % 2 == 0
    )
    if relayed:
        shared_shards = []
        for shard in (shared_gate, shared_up, shared_down):
            shared_shards += [shard, across_pairs(shard, tp_count)]
        scale_hi = lax.reduce_precision(route_weights, 8, 7)
        tables = jnp.stack([routes.astype(jnp.float32), scale_hi, route_weights - scale_hi])
        tables = tables.astype(jnp.bfloat16).reshape(-1, lanes)
        table_rows = tables.shape[0]
        tables = jnp.pad(tables, ((0, -table_rows % 16), (0, 0)))
        scaled = rotated_query * jnp.asarray(score_scale, jnp.bfloat16)
        everything, token_heads = attend(
            scaled.transpose(2, 1, 0).reshape(HEAD_SIZE, head_count * tok_count),
            jnp.concatenate([packed, tables], axis=0),
            head_gain.reshape(head_count, HEAD_SIZE),
            tok_count,
            sp_count // tp_count,
            tp_count,
            0,
        )
        tables = everything[:, tok_count : tok_count + table_rows]
    else:
        piece = exchange(packed, "sp", 0, True).reshape(sequence_total, lanes)
        query_rows = rotated_query.transpose(1, 0, 2).reshape(head_count * tok_count, HEAD_SIZE)
        block_length = key_block_rows(sequence_total)
        key_blocks = piece.reshape(sequence_total // block_length, block_length, lanes)
        attended = scan_attention(query_rows, key_blocks, score_scale)
        attended = attended.reshape(head_count, tok_count, HEAD_SIZE).transpose(1, 0, 2)
        head_out = final_norm(attended, head_gain.reshape(head_count, HEAD_SIZE))
        head_out = head_out.astype(jnp.bfloat16).reshape(tok_count, head_count * HEAD_SIZE)
    part_rows = tok_count // tp_count
    if not relayed:
        token_heads = exchange(
            head_out.reshape(tp_count, part_rows, head_count * HEAD_SIZE), "tp", 1, False
        )
        token_heads = token_heads.transpose(1, 0, 2).reshape(part_rows, -1)
    own_resid = lax.dynamic_slice_in_dim(residual, tp_index * part_rows, part_rows, 0)
    hidden_own = (
        own_resid.astype(jnp.float32)
        + jnp.dot(token_heads, out_proj, preferred_element_type=jnp.float32)
    ).astype(jnp.bfloat16)
    normed_own = final_norm(hidden_own.astype(jnp.float32), ffn_gain).astype(jnp.bfloat16)
    model_width = normed_own.shape[1]
    gate_local = expert_gate[0]
    up_local = expert_up[0]
    down_local = expert_down[0]
    if relayed:
        width = sp_count // tp_count
        sp_index = lax.axis_index("sp")
        stood_for = proxy_plane(tp_index) * width + sp_index % width
        block_tables = lax.dynamic_index_in_dim(tables, stood_for, 0, keepdims=False)
        block_tables = block_tables.astype(jnp.float32).reshape(3, tok_count, topk_count)
        group = width * tp_count
        plane_experts = (sp_index // width) * group + jnp.arange(group, dtype=jnp.int32)
        named = block_tables[0].astype(jnp.int32)[:, :, None] == plane_experts[None, None, :]
        rank = slot_ranks(jnp.any(named, axis=1))
        slots = jnp.arange(capacity, dtype=jnp.int32)
        select = (rank.T[:, None, :] == slots[None, :, None]).astype(jnp.bfloat16)

        def combine(part):
            scale = jnp.sum(jnp.where(named, block_tables[part][:, :, None], 0.0), axis=1)
            table = select * scale.T.astype(jnp.bfloat16)[:, None, :]
            return table.reshape(group * capacity, tok_count)

        combine_hi, combine_lo = combine(1), combine(2)
        arrived, *others = dispatch(
            normed_own, select, shared_shards, tp_count, width, tp_count, 2
        )
        produced = expert_block(
            arrived.reshape(sp_count * capacity, model_width), gate_local, up_local, down_local
        )
        every_shard = []
        for i in range(0, len(shared_shards), 2):
            every_shard += shared_shards[i : i + 2] + others[i : i + 2]
        routed, shared_out = give_back(
            produced.reshape(sp_count, capacity, model_width),
            combine_hi,
            combine_lo,
            normed_own,
            every_shard,
            tp_count,
            width,
            tp_count,
            3,
        )
        return (
            hidden_own.astype(jnp.float32) + (shared_out + routed.astype(jnp.float32))
        ).astype(jnp.bfloat16)
    normed = exchange(normed_own, "tp", 2, True).reshape(tok_count, model_width)
    slot_total = sp_count * capacity
    experts_here = jnp.arange(sp_count, dtype=jnp.int32) * tp_count + tp_index
    named = routes[:, :, None] == experts_here[None, None, :]
    member = jnp.any(named, axis=1)
    scale = jnp.sum(jnp.where(named, route_weights[:, :, None], 0.0), axis=1)
    rank = slot_ranks(member)
    slots = jnp.arange(capacity, dtype=jnp.int32)
    chosen = rank.T[:, None, :] == slots[None, :, None]
    select = chosen.astype(jnp.bfloat16).reshape(slot_total, tok_count)
    outgoing = jnp.dot(select, normed, preferred_element_type=jnp.float32).astype(jnp.bfloat16)
    arrived = exchange(outgoing.reshape(sp_count, capacity, model_width), "sp", 3, False)
    produced = expert_block(
        arrived.reshape(slot_total, model_width), gate_local, up_local, down_local
    )
    returned = exchange(produced.reshape(sp_count, capacity, model_width), "sp", 4, False).reshape(
        slot_total, model_width
    )
    combine = jnp.where(chosen, scale.T[:, None, :], 0.0).reshape(slot_total, tok_count)
    combine_hi = lax.reduce_precision(combine, 8, 7)
    combine_lo = (combine - combine_hi).astype(jnp.bfloat16)
    combine_hi = combine_hi.astype(jnp.bfloat16)

    def mix(weights):
        return lax.dot_general(
            weights, returned, (((0,), (0,)), ((), ())), preferred_element_type=jnp.float32
        )

    gate_part = jnp.dot(normed, shared_gate, preferred_element_type=jnp.float32)
    up_part = jnp.dot(normed, shared_up, preferred_element_type=jnp.float32)
    shared_inner = (jax.nn.silu(gate_part) * up_part).astype(jnp.bfloat16)
    shares = (
        jnp.dot(shared_inner, shared_down, preferred_element_type=jnp.float32)
        + mix(combine_hi)
        + mix(combine_lo)
    ).astype(jnp.bfloat16)
    shares = exchange(shares.reshape(tp_count, part_rows, model_width), "tp", 5, False)
    mixed_rows = jnp.sum(shares.astype(jnp.float32), axis=0)
    return (hidden_own.astype(jnp.float32) + mixed_rows).astype(jnp.bfloat16)


def solution(mesh):
    placed = (
        P("sp", "tp"),
        P("sp", "tp"),
        P("sp", "tp"),
        P(),
        P(),
        P("tp"),
        P(),
        P("sp", None),
        P(),
        P("sp", None),
        P("sp", None),
        P(("sp", "tp"), None, None),
        P(("sp", "tp"), None, None),
        P(("sp", "tp"), None, None),
        P(None, "tp"),
        P(None, "tp"),
        P("tp", None),
    )
    return jax.shard_map(
        local, mesh=mesh, in_specs=placed, out_specs=P(("sp", "tp"), None), check_vma=False
    )
```
